32 devices in a mesh: ep: 8 (over z, x), tp: 4 (over y, core).
Axes of the slice: x: 2, y: 2, z: 4, core: 2. Of those that a mesh axis runs over, the one named last changes fastest.
Arguments:
- mixer_rows: bfloat16 [1024, 2048], P('ep'), may hold values from -40 to 40
- mixer_gain: float32 [2048], replicated, may hold values from 0.1 to 1.9
- inner_weight: bfloat16 [2048, 1024], P(None, 'tp'), may hold values from -0.125 to 0.125
- gate_in_weight: bfloat16 [2048, 1024], P(None, 'tp'), may hold values from -0.125 to 0.125
- gate_out_weight: bfloat16 [2048, 1024], P(None, 'tp'), may hold values from -0.125 to 0.125
- conv_taps: float32 [3, 1024], P(None, 'tp'), may hold values from -3.5 to 3.5
- mixer_out_weight: bfloat16 [1024, 2048], P('tp'), may hold values from -0.1875 to 0.1875
- routed_rows: bfloat16 [2048, 2048], P('ep'), may hold values from -40 to 40
- routed_gain: float32 [2048], replicated, may hold values from 0.1 to 1.9
- route_ids: int32 [2048, 2], P('ep'), may hold values from 0 to 7, all different within a row; in each aligned block of 256 rows (0 to 255, 256 to 511, ...) at most 128 rows name the same one
- route_weights: float32 [2048, 2], P('ep'), may hold values from 0.25 to 1
- expert_gate: bfloat16 [8, 2048, 2048], P('ep', None, 'tp'), may hold values from -0.125 to 0.125
- expert_up: bfloat16 [8, 2048, 2048], P('ep', None, 'tp'), may hold values from -0.125 to 0.125
- expert_down: bfloat16 [8, 2048, 2048], P('ep', 'tp'), may hold values from -0.125 to 0.125
Outputs:
- mixer_output: bfloat16 [1024, 2048], P('ep')
- routed_output: bfloat16 [2048, 2048], P('ep')
The draws below stay inside these ranges and needn't reach their ends.
Inputs may be any that keep to these rules, and one draw needn't show every extreme that they name: `route_ids`: within each aligned block of 256 tokens, no expert is named by more than 128 choices, a bound that some block reaches; a token's 2 experts differ.
All inputs are finite; a program needn't handle non-finite values.
Results may differ from the reference program's by a relative error of at most 0.019.
Values may be sent and summed in bfloat16 or wider, within the bound.
A program may use at most 64 MiB of HBM per device.

```python
import math
import jax
import jax.numpy as jnp
import numpy as np
from jax import lax

D = 2048
CONV = 1024
TAPS = 3
FF = 2048
TOPK = 2
EXPERTS = 8
TOK2 = 256
TOKENS1 = 1024
TOKENS2 = 2048
CAP = 128
N_TP = 4


def scaled_rows(key, row_total, model_width):
    keys = jax.random.split(key, 3)
    row_scale = jnp.exp(jax.random.uniform(keys[0], (row_total, 1), jnp.float32) * math.log(10.0))
    col_scale = jnp.exp(jax.random.uniform(keys[1], (1, model_width), jnp.float32) * math.log(10.0))
    base = jnp.clip(jax.random.normal(keys[2], (row_total, model_width), jnp.float32), -4.0, 4.0)
    return (base * row_scale * col_scale * 0.1).astype(jnp.bfloat16)


def draw_mixer_rows(key, part):
    return scaled_rows(jax.random.fold_in(key, 11), TOKENS1, D)


def draw_routed_rows(key, part):
    return scaled_rows(jax.random.fold_in(key, 23), TOKENS2, D)


def steps_of(stream_key, shape, pieces, least, top_value):
    loudness, own = 1.0, jax.random.fold_in(stream_key, 6)
    for dim, blocks in pieces:
        steps = jnp.exp(jax.random.uniform(jax.random.fold_in(own, dim), (blocks,), jnp.float32, least / len(pieces), top_value / len(pieces)))
        loudness = loudness * jnp.repeat(steps, shape[dim] // blocks).reshape([-1 if axis == dim else 1 for axis in range(len(shape))])
    return loudness


def assign_block(stream_key, own, number, rows, count, top, most, lean):
    order = jax.random.permutation(stream_key, count)
    crowded, usual = load_shares(count, rows * top, most, lean, True), load_shares(count, rows * top, most, lean, False)
    places = jnp.arange(count)

    def named(sizes, turn):
        used = int((sizes > 0).sum())
        fixed = max(1, used // 4)
        passed = fixed + (places - fixed + turn * (used - fixed)) % max(1, count - fixed)
        return jnp.zeros((count,), jnp.int32).at[order[jnp.where(places < fixed, places, passed)]].set(jnp.asarray(sizes, jnp.int32))

    sizes = jnp.where(number % 4 == 0, named(crowded, number // 4), named(usual, number - number // 4 - 1))
    mixed = jax.random.permutation(jax.random.fold_in(own, 3), count)
    donor, taker = mixed[0:count // 2 * 2:2], mixed[1:count // 2 * 2:2]
    room = jnp.minimum(sizes[donor] - 1, most - sizes[taker]) // 2
    room = jnp.where((donor == order[0]) | (taker == order[0]) | (sizes[taker] == 0), 0, jnp.maximum(room, 0))
    passed = jax.random.randint(jax.random.fold_in(own, 4), (count // 2,), 0, 1 << 20) % (room + 1)
    sizes = sizes.at[donor].add(-passed).at[taker].add(passed)
    members = jnp.searchsorted(jnp.cumsum(sizes), jnp.arange(rows * top), side="right").astype(jnp.int32)
    listing = members.reshape(top, rows).T
    listing = listing[jax.random.permutation(jax.random.fold_in(own, 1), rows)]
    turn = jax.random.randint(jax.random.fold_in(own, 2), (rows, 1), 0, top)
    return jnp.take_along_axis(listing, (jnp.arange(top)[None, :] + turn) % top, axis=1)


def load_shares(number_of, total, limit, skew, full):
    loads = [(1 << 20) // math.isqrt(grade ** skew) + 1 for grade in range(1, number_of + 1)]
    largest = limit if full else min(limit, max(-(-total // number_of), total * loads[0] // sum(loads)))
    least = 1 if total - largest >= number_of - 1 else 0
    given, surplus = [largest] + [least] * (number_of - 1), total - largest - least * (number_of - 1)
    while surplus > 0:
        movable = [i for i in range(1, number_of) if given[i] < largest] or [i for i in range(1, number_of) if given[i] < limit]
        mass, left = sum([loads[i] for i in movable]), surplus
        for i in movable:
            extra = min(limit - given[i], max(1, left * loads[i] // mass), surplus)
            given[i] = given[i] + extra
            surplus = surplus - extra
    return np.array(given)


def noise(key, dims, scale, bound, cuts=(), kind=jnp.bfloat16):
    loudness = steps_of(key, dims, cuts, -0.22, 0.18) if cuts else 1.0
    entries = jax.random.normal(key, dims, jnp.float32) * scale * loudness
    return jnp.minimum(jnp.maximum(entries, -bound), bound).astype(kind)


def setup_inputs(seed: int = 0) -> dict:
    arg_keys = jax.random.split(jax.random.key(seed), 15)
    mixer_rows = draw_mixer_rows(jax.random.fold_in(arg_keys[14], 71), 0)
    mixer_gain = jnp.clip(1.0 + 0.18 * jax.random.normal(arg_keys[1], (D,), jnp.float32), 0.1, 1.9)
    inner_weight = noise(arg_keys[2], (D, CONV), D ** -0.5, 0.125, ((1, 4),))
    gate_in_weight = noise(arg_keys[3], (D, CONV), D ** -0.5, 0.125, ((1, 4),))
    gate_out_weight = noise(arg_keys[4], (D, CONV), D ** -0.5, 0.125, ((1, 4),))
    conv_taps = noise(arg_keys[5], (TAPS, CONV), TAPS ** -0.5, 3.5, ((1, 4),), jnp.float32)
    mixer_out_weight = noise(arg_keys[6], (CONV, D), CONV ** -0.5, 0.1875, ((0, 4),))
    routed_rows = draw_routed_rows(jax.random.fold_in(arg_keys[14], 71), 0)
    routed_gain = jnp.clip(1.0 + 0.18 * jax.random.normal(arg_keys[8], (D,), jnp.float32), 0.1, 1.9)
    route_ids_keys = jax.random.split(jax.random.fold_in(arg_keys[9], 1), TOKENS2 // TOK2)
    route_ids_turns = jax.random.permutation(jax.random.fold_in(arg_keys[9], 3), TOKENS2 // TOK2)
    route_ids = jax.vmap(lambda own, number: assign_block(jax.random.fold_in(arg_keys[9], 2), own, number, TOK2, EXPERTS, TOPK, CAP, 2))(route_ids_keys, route_ids_turns).reshape((TOKENS2, TOPK))
    route_weights = jnp.clip(0.25 + 0.75 * jax.random.uniform(arg_keys[10], (TOKENS2, TOPK), jnp.float32) ** steps_of(arg_keys[10], (TOKENS2, TOPK), ((0, 8),), -0.2, 0.2), 0.25, 1.0)
    expert_gate = noise(arg_keys[11], (EXPERTS, D, FF), D ** -0.5, 0.125, ((0, 8), (2, 4)))
    expert_up = noise(arg_keys[12], (EXPERTS, D, FF), D ** -0.5, 0.125, ((0, 8), (2, 4)))
    expert_down = noise(arg_keys[13], (EXPERTS, FF, D), FF ** -0.5, 0.125, ((0, 8), (1, 4)))
    return dict(mixer_rows=mixer_rows, mixer_gain=mixer_gain, inner_weight=inner_weight, gate_in_weight=gate_in_weight, gate_out_weight=gate_out_weight, conv_taps=conv_taps, mixer_out_weight=mixer_out_weight, routed_rows=routed_rows, routed_gain=routed_gain, route_ids=route_ids, route_weights=route_weights, expert_gate=expert_gate, expert_up=expert_up, expert_down=expert_down)


def rms_scale(row_block, gain_row):
    values = row_block.astype(jnp.float32)
    scaled = values * lax.rsqrt(lax.optimization_barrier(jnp.mean(values * values, axis=-1, keepdims=True)) + 1e-06)
    return (scaled * gain_row).astype(jnp.bfloat16)

def rounded_again(partial_value):
    return lax.optimization_barrier(partial_value.astype(jnp.bfloat16)).astype(jnp.float32)

def reference(mixer_rows, mixer_gain, inner_weight, gate_in_weight, gate_out_weight, conv_taps, mixer_out_weight, routed_rows, routed_gain, route_ids, route_weights, expert_gate, expert_up, expert_down):
    normed = rms_scale(mixer_rows, mixer_gain)
    inner_proj = jnp.dot(normed, inner_weight, preferred_element_type=jnp.float32)
    gate_in = jnp.dot(normed, gate_in_weight, preferred_element_type=jnp.float32)
    conv_input = (gate_in * inner_proj).astype(jnp.bfloat16)
    gate_out = jnp.dot(normed, gate_out_weight, preferred_element_type=jnp.float32)
    padded = jnp.concatenate([jnp.zeros((TAPS - 1, CONV), jnp.bfloat16), conv_input], axis=0).astype(jnp.float32)
    conv_out = jnp.zeros((TOKENS1, CONV), jnp.float32)
    for tap_index in range(TAPS):
        conv_out = conv_out + conv_taps[tap_index] * padded[tap_index:tap_index + TOKENS1]
    gated_conv = (gate_out * conv_out).astype(jnp.bfloat16)
    group_width = CONV // N_TP
    running = jnp.zeros((TOKENS1, D), jnp.float32)
    for piece_index in range(N_TP):
        lower_edge = piece_index * group_width
        partial_value = jnp.dot(gated_conv[:, lower_edge:lower_edge + group_width], mixer_out_weight[lower_edge:lower_edge + group_width], preferred_element_type=jnp.float32)
        running = running + rounded_again(partial_value)
    mixer_output = running.astype(jnp.bfloat16)
    routed_normed = rms_scale(routed_rows, routed_gain)
    blocks = TOKENS2 // TOK2
    flat_ids = route_ids.reshape(blocks, TOK2 * TOPK).astype(jnp.int32)
    onehot = (flat_ids[:, :, None] == jnp.arange(EXPERTS, dtype=jnp.int32)[None, None, :]).astype(jnp.int32)
    earlier = (jnp.cumsum(onehot, axis=1) - onehot).astype(jnp.int32)
    slot_rank = lax.optimization_barrier(jnp.sum(earlier * onehot, axis=2)).astype(jnp.int32)
    block_grid = jnp.broadcast_to(jnp.arange(blocks, dtype=jnp.int32)[:, None], flat_ids.shape)
    token_index = (block_grid * TOK2 + jnp.arange(TOK2 * TOPK, dtype=jnp.int32)[None, :] // TOPK).astype(jnp.int32)
    token_table = jnp.full((EXPERTS, blocks, CAP), TOKENS2, jnp.int32).at[flat_ids, block_grid, slot_rank].set(token_index)
    padded_rows = jnp.concatenate([routed_normed, jnp.zeros((1, D), jnp.bfloat16)], axis=0)
    hidden_width = FF // N_TP

    def one_expert(operands):
        table_rows, gate_w, up_w, down_w = operands
        slot_rows = padded_rows[table_rows.reshape(-1)]
        gate_act = jnp.dot(slot_rows, gate_w, preferred_element_type=jnp.float32)
        up_act = jnp.dot(slot_rows, up_w, preferred_element_type=jnp.float32)
        hidden = (jax.nn.silu(gate_act) * up_act).astype(jnp.bfloat16)
        summed = jnp.zeros((slot_rows.shape[0], D), jnp.float32)
        for piece_index in range(N_TP):
            lower_edge = piece_index * hidden_width
            partial_value = jnp.dot(hidden[:, lower_edge:lower_edge + hidden_width], down_w[lower_edge:lower_edge + hidden_width], preferred_element_type=jnp.float32)
            summed = summed + rounded_again(partial_value)
        return summed.astype(jnp.bfloat16)
    results = lax.map(one_expert, (token_table, expert_gate, expert_up, expert_down))
    results = results.reshape(EXPERTS, blocks, CAP, D)
    picked = results[flat_ids, block_grid, slot_rank].reshape(TOKENS2, TOPK, D).astype(jnp.float32)
    picked = picked * route_weights[:, :, None]
    owner_piece = (slot_rank // (CAP // N_TP)).reshape(TOKENS2, TOPK)
    running_two = jnp.zeros((TOKENS2, D), jnp.float32)
    for piece_index in range(N_TP):
        partial_value = lax.optimization_barrier(jnp.sum(jnp.where((owner_piece == piece_index)[:, :, None], picked, jnp.float32(0.0)), axis=1))
        running_two = running_two + rounded_again(partial_value)
    routed_output = running_two.astype(jnp.bfloat16)
    return (mixer_output, routed_output)
```

```python
import jax
import jax.numpy as jnp
from jax import lax
from jax.experimental import pallas as pl
from jax.experimental.pallas import tpu as pltpu
from jax.sharding import PartitionSpec as P

F32, BF16, I32 = jnp.float32, jnp.bfloat16, jnp.int32
CORES = 2


def rms(values):
    return lax.rsqrt(jnp.mean(values * values, axis=-1, keepdims=True) + 1e-06)


def dot(a, b):
    return jnp.dot(a, b, preferred_element_type=F32)


ORDER = (
    "W", "C00", "E00", "M", "N", "A01", "Aa0", "O", "C01", "E01",
    "Aa1", "Ba0", "Ca0", "Ea0", "A10", "Ab0", "P", "Ba1", "Ca1", "Ea1",
    "G00", "G01", "Ga0", "Ab1", "A11", "Bb0", "Cb0", "Eb0", "Ga1", "C10",
    "E10", "Bb1", "Cb1", "Gb0", "Eb1", "C11", "E11", "Gb1", "G10", "G11",
)
QUEUE = ("01", "20", "30", "21", "31", "10", "11")


def schedule(steps, per, whole):
    if steps == 4 and per == 2 and whole == 2:
        return 2, QUEUE, ORDER
    queue = [str(i) for i in range(steps)]
    order = ["M", "N", "W", "A00", "C00", "O", "E00", "P"]
    for last, i in zip(queue, queue[1:]):
        order += [name + i + "0" for name in ("AC" if int(i) < whole else "ABC") + "E"]
        order.append("G" + last + "0")
    return 1, [i + "0" for i in queue], order + ["G" + queue[-1] + "0"]


def make_kernel(
    experts, groups, tok, picks, width, cap, steps, per, mrows, taps_n, chan, hid, whole, halves, queue, order, pieces
):
    high = groups // CORES
    slab = width // groups
    wide = slab // pieces
    size = per // halves
    rows = size * cap
    edge = 16 * -(-(taps_n - 1) // 16)

    def kernel(
        mixer_h, mixer_gain_h, inner_h, gate_in_h, gate_out_h, taps_h, mixer_out_h,
        routed_h, routed_gain_h, ids_h, weights_h, gate_h, up_h, down_h,
        out_m, out_r,
        mixer_rows, mixer_gain, taps, routed_rows, routed_gain, ids, weights,
        w_inner, w_gin, w_gout, w_mout, w_gate, w_up, w_down,
        disp, slots, part, r1, s2, r2, t3, ret,
        rim, rim_in, m_part, m_r1, m_s2, m_r2,
        w_sem, own_sem,
        d1_s, d1_r, y_s, y_r, b_s, b_r, e_s, e_r, g_s, g_r, ret_s, ret_r,
        rim_s, rim_r, me_s, me_r, mg_s, mg_r, ay_s, ay_r, ab_s, ab_r,
    ):
        me = lax.axis_index("ep")
        t = lax.axis_index("tp")
        yy, cc = t // CORES, t % CORES
        mate = yy * CORES + (1 - cc)
        my_chunk, my_j = me // per, me % per
        sent = []

        def send(src, dst, ssem, rsem, where):
            copy = pltpu.make_async_remote_copy(
                src_ref=src, dst_ref=dst, send_sem=ssem, recv_sem=rsem,
                device_id=where, device_id_type=pl.DeviceIdType.MESH,
            )
            copy.start()
            sent.append(copy)

        def arrive(dst, ssem, rsem):
            pltpu.make_async_remote_copy(
                src_ref=dst, dst_ref=dst, send_sem=ssem, recv_sem=rsem,
                device_id={"tp": mate}, device_id_type=pl.DeviceIdType.MESH,
            ).wait_recv()

        def up_to(dy):
            return lax.rem(yy + dy, high)

        def down_to(dy):
            return lax.rem(yy + high - dy, high)

        barrier = pltpu.get_barrier_semaphore()
        for d in range(1, experts):
            pl.semaphore_signal(
                barrier, inc=1, device_id={"ep": lax.rem(me + d, experts)},
                device_id_type=pl.DeviceIdType.MESH,
            )
        for dy in range(1, high):
            pl.semaphore_signal(
                barrier, inc=1, device_id={"tp": up_to(dy) * CORES + cc},
                device_id_type=pl.DeviceIdType.MESH,
            )
        pl.semaphore_signal(
            barrier, inc=1, device_id={"tp": mate}, device_id_type=pl.DeviceIdType.MESH
        )

        loads = {}
        for place, (name, src, dst) in enumerate(
            (
                ("ids", ids_h, ids), ("weights", weights_h, weights),
                ("mixer", mixer_h, mixer_rows), ("mgain", mixer_gain_h, mixer_gain),
                ("gin", gate_in_h, w_gin), ("inner", inner_h, w_inner),
                ("routed", routed_h, routed_rows), ("rgain", routed_gain_h, routed_gain),
                ("taps", taps_h, taps), ("gout", gate_out_h, w_gout), ("mout", mixer_out_h, w_mout),
                ("gate", gate_h, w_gate), ("up", up_h, w_up), ("down", down_h, w_down),
            )
        ):
            loads[name] = pltpu.make_async_copy(src, dst, w_sem.at[place])
            loads[name].start()

        def loaded(*names):
            for name in names:
                loads[name].wait()

        with jax.named_scope("route"):
            loaded("ids", "weights")
            row = lax.broadcasted_iota(I32, (128, tok), 0)
            hits = [row == ids[k : k + 1, :] for k in range(picks)]
            named = sum(h.astype(F32) for h in hits)
            before = (
                lax.broadcasted_iota(I32, (tok, tok), 0) < lax.broadcasted_iota(I32, (tok, tok), 1)
            ).astype(F32).astype(BF16)
            earlier = dot(named.astype(BF16), before)
            slot_row = lax.broadcasted_iota(I32, (experts * cap, tok), 0)
            pick_map = jnp.zeros((experts * cap, tok), F32)
            sum_map = jnp.zeros((experts * cap, tok), F32)
            for k in range(picks):
                rank = jnp.sum(jnp.where(hits[k], earlier, 0.0), axis=0, keepdims=True).astype(I32)
                at = slot_row == (ids[k : k + 1, :] * cap + rank)
                pick_map = pick_map + jnp.where(at, 1.0, 0.0)
                sum_map = sum_map + jnp.where(at, weights[k : k + 1, :], 0.0)
            pick_map, sum_map = pick_map.astype(BF16), sum_map.astype(BF16)

        my_cols = pl.ds(pl.multiple_of(t * slab, slab), slab)

        with jax.named_scope("mix1"):
            loaded("mixer", "mgain", "gin", "inner")
            mixed = mixer_rows[...].astype(F32)
            mixed = ((mixed * rms(mixed)) * mixer_gain[...]).astype(BF16)
            conv_input = (dot(mixed, w_gin[...]) * dot(mixed, w_inner[...])).astype(BF16)
            rim[...] = conv_input[mrows - edge :]

        def pick(dy, scale):
            y = down_to(dy)
            cols = pl.ds(pl.multiple_of((y * CORES + cc) * slab, slab), slab)
            normed = ((routed_rows[:, cols].astype(F32) * scale) * routed_gain[:, cols]).astype(BF16)
            disp[dy] = dot(pick_map, normed).astype(BF16).reshape(experts, cap, slab)

        with jax.named_scope("pick"):
            loaded("routed", "rgain")
            scale = rms(routed_rows[...].astype(F32))
            pick(0, scale)

        with jax.named_scope("barrier"):
            pl.semaphore_wait(barrier, experts - 1 + high - 1 + 1)
        send(rim, rim_in, rim_s.at[0], rim_r.at[0], {"ep": lax.rem(me + 1, experts)})

        def blocks(h):
            return [lax.rem(my_j + h * size + n, per) for n in range(size)]

        def is_own(i, h, n):
            return i == "0" and h == 0 and n == 0

        outer = 1 - (my_chunk + 1) // 2 % 2
        index = {"a": 2 + outer, "b": 3 - outer}

        def at(i):
            return index[i] if i in index else int(i)

        def far(i):
            return i in index or int(i) >= whole

        def partner(i):
            chunk, other = my_chunk, at(i)
            for bit in (1 << n for n in range((steps - 1).bit_length())):
                chunk = chunk + other // bit % 2 * (bit - 2 * bit * lax.rem(chunk // bit, 2))
            return chunk

        def slabs(i):
            return range(1 if far(i) else high)

        def dispatch(i, h):
            for n, jj in enumerate(blocks(h)):
                if not is_own(i, h, n):
                    dest = partner(i) * per + jj
                    for dy in slabs(i):
                        send(
                            disp.at[dy, dest], slots.at[down_to(dy) * CORES + cc, at(i), my_j],
                            d1_s.at[at(i), jj, dy], d1_r.at[at(i), my_j, dy], {"ep": dest},
                        )

        own = []

        def keep(dy):
            block = slots.at[down_to(dy) * CORES + cc, 0, my_j]
            send(disp.at[dy, me], block, b_s.at[0, dy, my_j], b_r.at[0, dy, my_j], {"tp": mate})
            copy = pltpu.make_async_copy(disp.at[dy, me], block, own_sem.at[dy])
            copy.start()
            own.append(copy)

        with jax.named_scope("dispatch"):
            keep(0)
            for dy in range(1, high):
                pick(dy, scale)
                keep(dy)
            for word in queue:
                dispatch(word[0], int(word[1]))

        def stage_a(i, h):
            k = at(i)
            for n, jj in enumerate(blocks(h)):
                if is_own(i, h, n):
                    continue
                for dy in slabs(i):
                    block = slots.at[down_to(dy) * CORES + cc, k, jj]
                    arrive(block, d1_s.at[k, jj, dy], d1_r.at[k, jj, dy])
                    if far(i):
                        for up in range(1, high):
                            send(
                                block, block, y_s.at[k, up - 1, jj], y_r.at[k, up - 1, jj],
                                {"tp": up_to(up) * CORES + cc},
                            )
                    send(block, block, b_s.at[k, dy, jj], b_r.at[k, dy, jj], {"tp": mate})

        def stage_b(i, h):
            k = at(i)
            for dy in range(1, high):
                for jj in blocks(h):
                    block = slots.at[down_to(dy) * CORES + cc, k, jj]
                    arrive(block, y_s.at[k, dy - 1, jj], y_r.at[k, dy - 1, jj])
                    send(block, block, b_s.at[k, dy, jj], b_r.at[k, dy, jj], {"tp": mate})

        turns = list(range(1, high)) + [0]

        def columns(dy, core):
            return pl.ds(pl.multiple_of((up_to(dy) * CORES + core) * slab, slab), slab)

        def stage_c(i, h):
            k = at(i)
            for dy in range(high):
                for jj in blocks(h):
                    arrive(
                        slots.at[down_to(dy) * CORES + (1 - cc), k, jj],
                        b_s.at[k, dy, jj], b_r.at[k, dy, jj],
                    )
            if is_own(i, h, 0):
                for copy in own:
                    copy.wait()
            x = jnp.concatenate(
                [
                    jnp.concatenate([slots[q, k, jj] for q in range(groups)], axis=1)
                    for jj in blocks(h)
                ],
                axis=0,
            )
            gate, up = dot(x, w_gate[...]), dot(x, w_up[...])
            hidden = (gate / (1.0 + jnp.exp(-gate)) * up).astype(BF16)
            for side, core in ((0, 1 - cc), (1, cc)):
                for dy in turns:
                    value = dot(hidden, w_down[:, columns(dy, core)]).astype(BF16)
                    for p in range(pieces):
                        part[k, h, side, dy, p] = value[:, p * wide : (p + 1) * wide]
                        if side == 0:
                            send(
                                part.at[k, h, 0, dy, p], r1.at[k, h, dy, p],
                                e_s.at[k, h, dy, p], e_r.at[k, h, dy, p], {"tp": mate},
                            )

        def stage_e(i, h):
            k = at(i)
            for dy in range(1, high):
                for p in range(pieces):
                    arrive(r1.at[k, h, dy, p], e_s.at[k, h, dy, p], e_r.at[k, h, dy, p])
                    s2[k, h, dy - 1, p] = (
                        part[k, h, 1, dy, p].astype(F32) + r1[k, h, dy, p].astype(F32)
                    ).astype(BF16)
                    send(
                        s2.at[k, h, dy - 1, p], r2.at[k, h, dy - 1, p],
                        g_s.at[k, h, dy - 1, p], g_r.at[k, h, dy - 1, p],
                        {"tp": up_to(dy) * CORES + cc},
                    )

        def stage_g(i, h):
            k = at(i)
            for p in range(pieces):
                arrive(r1.at[k, h, 0, p], e_s.at[k, h, 0, p], e_r.at[k, h, 0, p])
                total = part[k, h, 1, 0, p].astype(F32) + r1[k, h, 0, p].astype(F32)
                for dy in range(1, high):
                    arrive(r2.at[k, h, dy - 1, p], g_s.at[k, h, dy - 1, p], g_r.at[k, h, dy - 1, p])
                    total = total + r2[k, h, dy - 1, p].astype(F32)
                t3[k, h, p] = total.astype(BF16).reshape(size, cap, wide)
                for n, jj in enumerate(blocks(h)):
                    if is_own(i, h, n):
                        ret[p, me] = t3[k, h, p, n]
                        continue
                    dest = partner(i) * per + jj
                    send(
                        t3.at[k, h, p, n], ret.at[p, me], ret_s.at[k, h, p, n], ret_r.at[p, me],
                        {"ep": dest},
                    )

        def window_of(out, group, p, count):
            span = slab // count
            return out.at[:, pl.ds(pl.multiple_of(group * slab + p * span, span), span)]

        def spread(which, out, p, count, value):
            span = slab // count
            out[:, pl.ds(pl.multiple_of(t * slab + p * span, span), span)] = value
            window = window_of(out, t, p, count)
            for dy in range(1, high):
                send(
                    window, window, ay_s.at[which, dy - 1, p], ay_r.at[which, dy - 1, p],
                    {"tp": up_to(dy) * CORES + cc},
                )
            send(window, window, ab_s.at[which, 0, p], ab_r.at[which, 0, p], {"tp": mate})

        def spread_on(which, out, p, count):
            for dy in range(1, high):
                window = window_of(out, down_to(dy) * CORES + cc, p, count)
                arrive(window, ay_s.at[which, dy - 1, p], ay_r.at[which, dy - 1, p])
                send(window, window, ab_s.at[which, dy, p], ab_r.at[which, dy, p], {"tp": mate})

        def spread_end(which, out, p, count):
            for dy in range(high):
                arrive(
                    window_of(out, down_to(dy) * CORES + (1 - cc), p, count),
                    ab_s.at[which, dy, p], ab_r.at[which, dy, p],
                )

        def mixer_out():
            loaded("gout", "taps")
            gate_out = dot(mixed, w_gout[...])
            arrive(rim_in, rim_s.at[0], rim_r.at[0])
            first = jnp.where(me == 0, 0.0, rim_in[...].astype(F32))
            extended = jnp.concatenate([first, conv_input.astype(F32)], axis=0)
            conv = jnp.zeros((mrows, chan), F32)
            for k in range(taps_n):
                start = edge - (taps_n - 1) + k
                conv = conv + taps[k : k + 1, :] * extended[start : start + mrows]
            gated = (gate_out * conv).astype(BF16)
            loaded("mout")
            for side, core in ((0, 1 - cc), (1, cc)):
                for dy in turns:
                    m_part[side, dy] = dot(gated, w_mout[:, columns(dy, core)]).astype(BF16)
                    if side == 0:
                        send(m_part.at[0, dy], m_r1.at[dy], me_s.at[dy], me_r.at[dy], {"tp": mate})

        def mixer_pair():
            for dy in range(1, high):
                arrive(m_r1.at[dy], me_s.at[dy], me_r.at[dy])
                m_s2[dy - 1] = (m_part[1, dy].astype(F32) + m_r1[dy].astype(F32)).astype(BF16)
                send(
                    m_s2.at[dy - 1], m_r2.at[dy - 1], mg_s.at[dy - 1], mg_r.at[dy - 1],
                    {"tp": up_to(dy) * CORES + cc},
                )

        def mixer_sum():
            arrive(m_r1.at[0], me_s.at[0], me_r.at[0])
            total = m_part[1, 0].astype(F32) + m_r1[0].astype(F32)
            for dy in range(1, high):
                arrive(m_r2.at[dy - 1], mg_s.at[dy - 1], mg_r.at[dy - 1])
                total = total + m_r2[dy - 1].astype(F32)
            spread(0, out_m, 0, 1, total.astype(BF16))

        def finish(p):
            for d in range(1, experts):
                e = lax.rem(me + d, experts)
                arrive(ret.at[p, e], ret_s.at[0, 0, 0, 0], ret_r.at[p, e])
            summed = lax.dot_general(
                sum_map, ret[p].reshape(experts * cap, wide), (((0,), (0,)), ((), ())),
                preferred_element_type=F32,
            )
            spread(1, out_r, p, pieces, summed.astype(BF16))

        stages = dict(
            M=mixer_out, N=mixer_pair, O=mixer_sum, P=lambda: spread_on(0, out_m, 0, 1),
            W=lambda: loaded("gate", "up", "down"),
            A=stage_a, B=stage_b, C=stage_c, E=stage_e, G=stage_g,
        )
        for word in order:
            with jax.named_scope(word):
                stages[word[0]](*((word[1], int(word[2:])) if word[1:] else ()))
        early = sent[: 2 * len(sent) // 3]
        for copy in early:
            copy.wait_send()
        with jax.named_scope("finish"):
            for p in range(pieces):
                finish(p)
        with jax.named_scope("spreadon"):
            for p in range(pieces):
                spread_on(1, out_r, p, pieces)
        with jax.named_scope("end"):
            spread_end(0, out_m, 0, 1)
            for p in range(pieces):
                spread_end(1, out_r, p, pieces)
        for copy in sent[len(early) :]:
            copy.wait_send()

    dma = pltpu.SemaphoreType.DMA
    far = max(1, high - 1)
    v = lambda *shape: pltpu.VMEM(shape, BF16)
    f = lambda *shape: pltpu.VMEM(shape, F32)
    scratch = [
        v(mrows, width), f(1, width), f(taps_n, chan), v(tok, width), f(1, width),
        pltpu.VMEM((picks, tok), I32), f(picks, tok),
        v(width, chan), v(width, chan), v(width, chan), v(chan, width),
        v(width, hid), v(width, hid), v(hid, width),
        v(high, experts, cap, slab), v(groups, steps, per, cap, slab),
        v(steps, halves, 2, high, pieces, rows, wide), v(steps, halves, high, pieces, rows, wide),
        v(steps, halves, far, pieces, rows, wide), v(steps, halves, far, pieces, rows, wide),
        v(steps, halves, pieces, size, cap, wide), v(pieces, experts, cap, wide),
        v(edge, chan), v(edge, chan),
        v(2, high, mrows, slab), v(high, mrows, slab), v(far, mrows, slab), v(far, mrows, slab),
        dma((14,)), dma((high,)),
        dma((steps, per, high)), dma((steps, per, high)),
        dma((steps, far, per)), dma((steps, far, per)),
        dma((steps, high, per)), dma((steps, high, per)),
        dma((steps, halves, high, pieces)), dma((steps, halves, high, pieces)),
        dma((steps, halves, far, pieces)), dma((steps, halves, far, pieces)),
        dma((steps, halves, pieces, size)), dma((pieces, experts)),
        dma((1,)), dma((1,)),
        dma((high,)), dma((high,)), dma((far,)), dma((far,)),
        dma((2, far, pieces)), dma((2, far, pieces)), dma((2, high, pieces)), dma((2, high, pieces)),
    ]
    return kernel, scratch


def store(a, b, out_a, out_b, sem):
    copies = [
        pltpu.make_async_copy(a, out_a, sem.at[0]), pltpu.make_async_copy(b, out_b, sem.at[1])
    ]
    for copy in copies:
        copy.start()
    for copy in copies:
        copy.wait()


def on_device(
    mixer_rows, mixer_gain, inner_weight, gate_in_weight, gate_out_weight, conv_taps,
    mixer_out_weight, routed_rows, routed_gain, route_ids, route_weights,
    expert_gate, expert_up, expert_down,
):
    experts, groups = lax.axis_size("ep"), lax.axis_size("tp")
    tok, picks = route_ids.shape
    width = routed_rows.shape[1]
    cap = 2 * tok * picks // experts
    per = max(1, min(experts, tok // cap))
    steps = experts // per
    mrows = mixer_rows.shape[0]
    taps_n, chan = conv_taps.shape
    whole = 2 if groups // CORES == 2 else 1
    pieces = max(1, min(2, width // groups // 256))
    kernel, scratch = make_kernel(
        experts, groups, tok, picks, width, cap, steps, per, mrows, taps_n, chan,
        expert_gate.shape[2], whole, *schedule(steps, per, whole), pieces,
    )
    near, far = pl.BlockSpec(memory_space=pltpu.VMEM), pl.BlockSpec(memory_space=pl.ANY)
    done = pl.pallas_call(
        kernel,
        out_shape=(pltpu.VMEM(mixer_rows.shape, BF16), pltpu.VMEM(routed_rows.shape, BF16)),
        in_specs=[far] * 14,
        out_specs=(near, near),
        scratch_shapes=scratch,
        compiler_params=pltpu.CompilerParams(
            collective_id=0, has_side_effects=True, vmem_limit_bytes=60 * 1024 * 1024
        ),
        name="mixer_and_experts",
    )(
        mixer_rows, mixer_gain[None, :], inner_weight, gate_in_weight, gate_out_weight, conv_taps,
        mixer_out_weight, routed_rows, routed_gain[None, :], route_ids.T, route_weights.T,
        expert_gate[0], expert_up[0], expert_down[0],
    )
    return pl.pallas_call(
        store,
        out_shape=(
            jax.ShapeDtypeStruct(mixer_rows.shape, BF16),
            jax.ShapeDtypeStruct(routed_rows.shape, BF16),
        ),
        in_specs=[far, far],
        out_specs=(far, far),
        scratch_shapes=[pltpu.SemaphoreType.DMA((2,))],
        name="store",
    )(*(pltpu.with_memory_space_constraint(array, pltpu.VMEM) for array in done))


def solution(mesh):
    return jax.shard_map(
        on_device,
        mesh=mesh,
        in_specs=(
            P("ep", None), P(), P(None, "tp"), P(None, "tp"), P(None, "tp"), P(None, "tp"),
            P("tp", None), P("ep", None), P(), P("ep", None), P("ep", None),
            P("ep", None, "tp"), P("ep", None, "tp"), P("ep", "tp", None),
        ),
        out_specs=(P("ep", None), P("ep", None)),
        check_vma=False,
    )
```

```python
import jax
import jax.numpy as jnp
from jax import lax
from jax.experimental import pallas as pl
from jax.experimental.pallas import tpu as pltpu
from jax.sharding import PartitionSpec as P

F32, BF16, I32 = jnp.float32, jnp.bfloat16, jnp.int32
CORES = 2


def rms(values):
    return lax.rsqrt(jnp.mean(values * values, axis=-1, keepdims=True) + 1e-06)


def dot(a, b):
    return jnp.dot(a, b, preferred_element_type=F32)


ORDER = (
    "W", "C00", "E00", "M", "N", "A01", "Aa0", "O", "C01", "E01",
    "T", "Aa1", "Ba0", "Ca0", "Ea0", "A10", "Ab0", "P", "Ba1", "Ca1",
    "Ea1", "G00", "G01", "Ga0", "Ab1", "A11", "Bb0", "Cb0", "Eb0", "Ga1",
    "C10", "E10", "Bb1", "Cb1", "Gb00", "Eb1", "C11", "E11", "Gb10", "G100",
    "Gb01", "Gb11", "G110", "G101", "G111",
)
QUEUE = ("01", "20", "30", "21", "31", "10", "11")
KINDS = ("d1", "y", "b", "e", "g", "ret", "rim", "me", "mg", "ay", "ab")


def schedule(steps, per, whole):
    if steps == 4 and per == 2 and whole == 2:
        return 2, QUEUE, ORDER
    queue = [str(i) for i in range(steps)]
    order = ["M", "N", "T", "W", "A00", "C00", "O", "E00", "P"]
    for last, i in zip(queue, queue[1:]):
        order += [name + i + "0" for name in ("AC" if int(i) < whole else "ABC") + "E"]
        order.append("G" + last + "0")
    return 1, [i + "0" for i in queue], order + ["G" + queue[-1] + "0"]


def make_kernel(
    experts, groups, tok, picks, width, cap, steps, per, mrows, taps_n, chan, hid, whole, halves, queue, order, pieces
):
    high = groups // CORES
    slab = width // groups
    wide = slab // pieces
    size = per // halves
    rows = size * cap
    edge = 16 * -(-(taps_n - 1) // 16)

    def kernel(
        mixer_h, mixer_gain_h, inner_h, gate_in_h, gate_out_h, taps_h, mixer_out_h,
        routed_h, routed_gain_h, ids_h, weights_h, gate_h, up_h, down_h,
        out_m, out_r,
        mixer_rows, mixer_gain, taps, routed_rows, routed_gain, ids, weights,
        w_inner, w_gin, w_gout, w_mout, w_gate, w_up, w_down,
        disp, slots, part, r1, s2, r2, t3, ret,
        sums,
        rim, rim_in, m_part, m_r1, m_s2, m_r2,
        w_sem, own_sem, s_sem,
        d1_r, y_r, b_r, e_r, g_r, ret_r,
        rim_r, me_r, mg_r, ay_r, ab_r,
    ):
        me = lax.axis_index("ep")
        t = lax.axis_index("tp")
        yy, cc = t // CORES, t % CORES
        mate = yy * CORES + (1 - cc)
        my_chunk, my_j = me // per, me % per
        sent = {}

        def send(src, dst, kind, rsem, where):
            copy = pltpu.make_async_remote_copy(
                src_ref=src, dst_ref=dst, send_sem=s_sem.at[KINDS.index(kind)], recv_sem=rsem,
                device_id=where, device_id_type=pl.DeviceIdType.MESH,
            )
            copy.start()
            sent[kind] = sent.get(kind, 0) + volume(src.shape)

        def volume(shape):
            total = 1
            for n in shape:
                total *= n
            return total

        def carrier(count):
            for ref in (gate_h, disp, slots, part):
                line = volume(ref.shape[1:])
                if count % line == 0 and count // line <= ref.shape[0]:
                    return ref.at[0 : count // line]
            for ref in (disp, slots):
                for a in range(1, ref.shape[0] + 1):
                    line = a * volume(ref.shape[2:])
                    if count % line == 0 and count // line <= ref.shape[1]:
                        return ref.at[0:a, 0 : count // line]
            raise ValueError(count)

        def drain(*kinds):
            for kind in kinds:
                if kind in sent:
                    ref = carrier(sent.pop(kind))
                    pltpu.make_async_remote_copy(
                        src_ref=ref, dst_ref=ref, send_sem=s_sem.at[KINDS.index(kind)],
                        recv_sem=s_sem.at[KINDS.index(kind)],
                        device_id={"tp": mate}, device_id_type=pl.DeviceIdType.MESH,
                    ).wait_send()

        def arrive(dst, rsem):
            pltpu.make_async_remote_copy(
                src_ref=dst, dst_ref=dst, send_sem=s_sem.at[0], recv_sem=rsem,
                device_id={"tp": mate}, device_id_type=pl.DeviceIdType.MESH,
            ).wait_recv()

        def up_to(dy):
            return lax.rem(yy + dy, high)

        def down_to(dy):
            return lax.rem(yy + high - dy, high)

        barrier = pltpu.get_barrier_semaphore()
        for d in range(1, experts):
            pl.semaphore_signal(
                barrier, inc=1, device_id={"ep": lax.rem(me + d, experts)},
                device_id_type=pl.DeviceIdType.MESH,
            )
        for dy in range(1, high):
            pl.semaphore_signal(
                barrier, inc=1, device_id={"tp": up_to(dy) * CORES + cc},
                device_id_type=pl.DeviceIdType.MESH,
            )
        pl.semaphore_signal(
            barrier, inc=1, device_id={"tp": mate}, device_id_type=pl.DeviceIdType.MESH
        )

        loads = {}
        for place, (name, src, dst) in enumerate(
            (
                ("ids", ids_h, ids), ("weights", weights_h, weights),
                ("mixer", mixer_h, mixer_rows), ("mgain", mixer_gain_h, mixer_gain),
                ("gin", gate_in_h, w_gin), ("inner", inner_h, w_inner),
                ("routed", routed_h, routed_rows), ("rgain", routed_gain_h, routed_gain),
                ("taps", taps_h, taps), ("gout", gate_out_h, w_gout), ("mout", mixer_out_h, w_mout),
                ("gate", gate_h, w_gate), ("up", up_h, w_up), ("down", down_h, w_down),
            )
        ):
            loads[name] = pltpu.make_async_copy(src, dst, w_sem.at[place])
            loads[name].start()

        def loaded(*names):
            for name in names:
                loads[name].wait()

        with jax.named_scope("route"):
            loaded("ids", "weights")
            row = lax.broadcasted_iota(I32, (128, tok), 0)
            hits = [row == ids[k : k + 1, :] for k in range(picks)]
            named = sum(h.astype(F32) for h in hits)
            before = (
                lax.broadcasted_iota(I32, (tok, tok), 0) < lax.broadcasted_iota(I32, (tok, tok), 1)
            ).astype(F32).astype(BF16)
            earlier = dot(named.astype(BF16), before)
            slot_row = lax.broadcasted_iota(I32, (experts * cap, tok), 0)
            pick_map = jnp.zeros((experts * cap, tok), F32)
            placed = []
            for k in range(picks):
                rank = jnp.sum(jnp.where(hits[k], earlier, 0.0), axis=0, keepdims=True).astype(I32)
                placed.append(ids[k : k + 1, :] * cap + rank)
                pick_map = pick_map + jnp.where(slot_row == placed[k], 1.0, 0.0)
            pick_map = pick_map.astype(BF16)

        def weigh():
            slot_row = lax.broadcasted_iota(I32, (experts * cap, tok), 0)
            total = jnp.zeros((experts * cap, tok), F32)
            for k in range(picks):
                total = total + jnp.where(slot_row == placed[k], weights[k : k + 1, :], 0.0)
            sums[...] = total.T.astype(BF16)

        my_cols = pl.ds(pl.multiple_of(t * slab, slab), slab)

        with jax.named_scope("mix1"):
            loaded("mixer", "mgain", "gin", "inner")
            mixed = mixer_rows[...].astype(F32)
            mixed = ((mixed * rms(mixed)) * mixer_gain[...]).astype(BF16)
            conv_input = (dot(mixed, w_gin[...]) * dot(mixed, w_inner[...])).astype(BF16)
            rim[...] = conv_input[mrows - edge :]

        def pick(dy, scale):
            y = down_to(dy)
            cols = pl.ds(pl.multiple_of((y * CORES + cc) * slab, slab), slab)
            normed = ((routed_rows[:, cols].astype(F32) * scale) * routed_gain[:, cols]).astype(BF16)
            disp[dy] = dot(pick_map, normed).astype(BF16).reshape(experts, cap, slab)

        with jax.named_scope("pick"):
            loaded("routed", "rgain")
            scale = rms(routed_rows[...].astype(F32))
            pick(0, scale)

        with jax.named_scope("barrier"):
            pl.semaphore_wait(barrier, experts - 1 + high - 1 + 1)
        send(rim, rim_in, "rim", rim_r.at[0], {"ep": lax.rem(me + 1, experts)})

        def blocks(h):
            return [lax.rem(my_j + h * size + n, per) for n in range(size)]

        def is_own(i, h, n):
            return i == "0" and h == 0 and n == 0

        outer = 1 - (my_chunk + 1) // 2 % 2
        index = {"a": 2 + outer, "b": 3 - outer}

        def at(i):
            return index[i] if i in index else int(i)

        def far(i):
            return i in index or int(i) >= whole

        def partner(i):
            chunk, other = my_chunk, at(i)
            for bit in (1 << n for n in range((steps - 1).bit_length())):
                chunk = chunk + other // bit % 2 * (bit - 2 * bit * lax.rem(chunk // bit, 2))
            return chunk

        def slabs(i):
            return range(1 if far(i) else high)

        def dispatch(i, h):
            for n, jj in enumerate(blocks(h)):
                if not is_own(i, h, n):
                    dest = partner(i) * per + jj
                    for dy in slabs(i):
                        send(disp.at[dy, dest], slots.at[down_to(dy) * CORES + cc, at(i), my_j], "d1", d1_r.at[at(i), my_j], {"ep": dest})

        own = []

        def keep(dy):
            block = slots.at[down_to(dy) * CORES + cc, 0, my_j]
            send(disp.at[dy, me], block, "b", b_r.at[0, 0], {"tp": mate})
            copy = pltpu.make_async_copy(disp.at[dy, me], block, own_sem.at[dy])
            copy.start()
            own.append(copy)

        with jax.named_scope("dispatch"):
            keep(0)
            for dy in range(1, high):
                pick(dy, scale)
                keep(dy)
            for word in queue:
                dispatch(word[0], int(word[1]))

        def stage_a(i, h):
            k = at(i)
            for n, jj in enumerate(blocks(h)):
                if is_own(i, h, n):
                    continue
                arrive(slots.at[0 : len(slabs(i)), k, jj], d1_r.at[k, jj])
                for dy in slabs(i):
                    block = slots.at[down_to(dy) * CORES + cc, k, jj]
                    if far(i):
                        for up in range(1, high):
                            send(
                                block, block, "y", y_r.at[k, up - 1, jj], {"tp": up_to(up) * CORES + cc}
                            )
                    send(block, block, "b", b_r.at[k, h], {"tp": mate})

        def stage_b(i, h):
            k = at(i)
            for dy in range(1, high):
                for jj in blocks(h):
                    block = slots.at[down_to(dy) * CORES + cc, k, jj]
                    arrive(block, y_r.at[k, dy - 1, jj])
                    send(block, block, "b", b_r.at[k, h], {"tp": mate})

        turns = list(range(1, high)) + [0]

        def columns(dy, core):
            return pl.ds(pl.multiple_of((up_to(dy) * CORES + core) * slab, slab), slab)

        def stage_c(i, h):
            k = at(i)
            arrive(slots.at[0:high, k, 0:size], b_r.at[k, h])
            if is_own(i, h, 0):
                for copy in own:
                    copy.wait()
            x = jnp.concatenate(
                [
                    jnp.concatenate([slots[q, k, jj] for q in range(groups)], axis=1)
                    for jj in blocks(h)
                ],
                axis=0,
            )
            gate, up = dot(x, w_gate[...]), dot(x, w_up[...])
            hidden = (gate / (1.0 + jnp.exp(-gate)) * up).astype(BF16)
            for side, core in ((0, 1 - cc), (1, cc)):
                for dy in turns:
                    value = dot(hidden, w_down[:, columns(dy, core)]).astype(BF16)
                    for p in range(pieces):
                        part[k, h, side, dy, p] = value[:, p * wide : (p + 1) * wide]
                    if side == 0:
                        send(part.at[k, h, 0, dy], r1.at[k, h, dy], "e", e_r.at[k, h, dy], {"tp": mate})

        def stage_e(i, h):
            k = at(i)
            for dy in range(1, high):
                arrive(r1.at[k, h, dy], e_r.at[k, h, dy])
                for p in range(pieces):
                    s2[k, h, dy - 1, p] = (
                        part[k, h, 1, dy, p].astype(F32) + r1[k, h, dy, p].astype(F32)
                    ).astype(BF16)
                    send(
                        s2.at[k, h, dy - 1, p], r2.at[k, h, dy - 1, p], "g", g_r.at[k, h, dy - 1, p],
                        {"tp": up_to(dy) * CORES + cc},
                    )

        def stage_g(i, h, *only):
            k = at(i)
            for p in only or range(pieces):
                if p == 0:
                    arrive(r1.at[k, h, 0], e_r.at[k, h, 0])
                total = part[k, h, 1, 0, p].astype(F32) + r1[k, h, 0, p].astype(F32)
                for dy in range(1, high):
                    arrive(r2.at[k, h, dy - 1, p], g_r.at[k, h, dy - 1, p])
                    total = total + r2[k, h, dy - 1, p].astype(F32)
                t3[k, h, p] = total.astype(BF16).reshape(size, cap, wide)
                for n, jj in enumerate(blocks(h)):
                    if is_own(i, h, n):
                        ret[p, me] = t3[k, h, p, n]
                        continue
                    dest = partner(i) * per + jj
                    send(t3.at[k, h, p, n], ret.at[p, me], "ret", ret_r.at[p], {"ep": dest})

        def window_of(out, group, p, count):
            span = slab // count
            return out.at[:, pl.ds(pl.multiple_of(group * slab + p * span, span), span)]

        def spread(which, out, p, count, value):
            span = slab // count
            out[:, pl.ds(pl.multiple_of(t * slab + p * span, span), span)] = value
            window = window_of(out, t, p, count)
            for dy in range(1, high):
                send(window, window, "ay", ay_r.at[which, dy - 1, p], {"tp": up_to(dy) * CORES + cc})
            send(window, window, "ab", ab_r.at[which], {"tp": mate})

        def spread_on(which, out, p, count):
            for dy in range(1, high):
                window = window_of(out, down_to(dy) * CORES + cc, p, count)
                arrive(window, ay_r.at[which, dy - 1, p])
                send(window, window, "ab", ab_r.at[which], {"tp": mate})

        def spread_end(which, out):
            arrive(out.at[:, pl.ds(0, high * slab)], ab_r.at[which])

        def mixer_out():
            loaded("gout", "taps")
            gate_out = dot(mixed, w_gout[...])
            arrive(rim_in, rim_r.at[0])
            first = jnp.where(me == 0, 0.0, rim_in[...].astype(F32))
            extended = jnp.concatenate([first, conv_input.astype(F32)], axis=0)
            conv = jnp.zeros((mrows, chan), F32)
            for k in range(taps_n):
                start = edge - (taps_n - 1) + k
                conv = conv + taps[k : k + 1, :] * extended[start : start + mrows]
            gated = (gate_out * conv).astype(BF16)
            loaded("mout")
            for side, core in ((0, 1 - cc), (1, cc)):
                for dy in turns:
                    m_part[side, dy] = dot(gated, w_mout[:, columns(dy, core)]).astype(BF16)
                    if side == 0:
                        send(m_part.at[0, dy], m_r1.at[dy], "me", me_r.at[dy], {"tp": mate})

        def mixer_pair():
            for dy in range(1, high):
                arrive(m_r1.at[dy], me_r.at[dy])
                m_s2[dy - 1] = (m_part[1, dy].astype(F32) + m_r1[dy].astype(F32)).astype(BF16)
                send(m_s2.at[dy - 1], m_r2.at[dy - 1], "mg", mg_r.at[dy - 1], {"tp": up_to(dy) * CORES + cc})

        def mixer_sum():
            arrive(m_r1.at[0], me_r.at[0])
            total = m_part[1, 0].astype(F32) + m_r1[0].astype(F32)
            for dy in range(1, high):
                arrive(m_r2.at[dy - 1], mg_r.at[dy - 1])
                total = total + m_r2[dy - 1].astype(F32)
            spread(0, out_m, 0, 1, total.astype(BF16))

        def finish(p):
            arrive(ret.at[p, 0 : experts - 1], ret_r.at[p])
            total = dot(sums[...], ret[p].reshape(experts * cap, wide))
            spread(1, out_r, p, pieces, total.astype(BF16))

        stages = dict(
            M=mixer_out, N=mixer_pair, O=mixer_sum, P=lambda: spread_on(0, out_m, 0, 1),
            W=lambda: loaded("gate", "up", "down"), T=weigh,
            A=stage_a, B=stage_b, C=stage_c, E=stage_e, G=stage_g,
        )
        for word in order:
            with jax.named_scope(word):
                stages[word[0]](*((word[1], *(int(c) for c in word[2:])) if word[1:] else ()))
        with jax.named_scope("early"):
            drain("d1", "y", "b", "e", "rim", "me", "mg")
        for p in range(pieces):
            with jax.named_scope("finish%d" % p):
                finish(p)
        with jax.named_scope("spreadon"):
            drain("g", "ret")
            for p in range(pieces):
                spread_on(1, out_r, p, pieces)
        with jax.named_scope("end"):
            spread_end(0, out_m)
            spread_end(1, out_r)
        with jax.named_scope("drain"):
            drain("ay", "ab")

    dma = pltpu.SemaphoreType.DMA
    far = max(1, high - 1)
    v = lambda *shape: pltpu.VMEM(shape, BF16)
    f = lambda *shape: pltpu.VMEM(shape, F32)
    scratch = [
        v(mrows, width), f(1, width), f(taps_n, chan), v(tok, width), f(1, width),
        pltpu.VMEM((picks, tok), I32), f(picks, tok),
        v(width, chan), v(width, chan), v(width, chan), v(chan, width),
        v(width, hid), v(width, hid), v(hid, width),
        v(high, experts, cap, slab), v(groups, steps, per, cap, slab),
        v(steps, halves, 2, high, pieces, rows, wide), v(steps, halves, high, pieces, rows, wide),
        v(steps, halves, far, pieces, rows, wide), v(steps, halves, far, pieces, rows, wide),
        v(steps, halves, pieces, size, cap, wide), v(pieces, experts, cap, wide),
        v(tok, experts * cap),
        v(edge, chan), v(edge, chan),
        v(2, high, mrows, slab), v(high, mrows, slab), v(far, mrows, slab), v(far, mrows, slab),
        dma((14,)), dma((high,)), dma((len(KINDS),)),
        dma((steps, per)), dma((steps, far, per)), dma((steps, halves)),
        dma((steps, halves, high)), dma((steps, halves, far, pieces)), dma((pieces,)),
        dma((1,)), dma((high,)), dma((far,)), dma((2, far, pieces)), dma((2,)),
    ]
    return kernel, scratch


def store(a, b, out_a, out_b, sem):
    copies = [
        pltpu.make_async_copy(a, out_a, sem.at[0]), pltpu.make_async_copy(b, out_b, sem.at[1])
    ]
    for copy in copies:
        copy.start()
    for copy in copies:
        copy.wait()


def on_device(
    mixer_rows, mixer_gain, inner_weight, gate_in_weight, gate_out_weight, conv_taps,
    mixer_out_weight, routed_rows, routed_gain, route_ids, route_weights,
    expert_gate, expert_up, expert_down,
):
    experts, groups = lax.axis_size("ep"), lax.axis_size("tp")
    tok, picks = route_ids.shape
    width = routed_rows.shape[1]
    cap = 2 * tok * picks // experts
    per = max(1, min(experts, tok // cap))
    steps = experts // per
    mrows = mixer_rows.shape[0]
    taps_n, chan = conv_taps.shape
    whole = 2 if groups // CORES == 2 else 1
    pieces = max(1, min(2, width // groups // 256))
    kernel, scratch = make_kernel(
        experts, groups, tok, picks, width, cap, steps, per, mrows, taps_n, chan,
        expert_gate.shape[2], whole, *schedule(steps, per, whole), pieces,
    )
    near, far = pl.BlockSpec(memory_space=pltpu.VMEM), pl.BlockSpec(memory_space=pl.ANY)
    done = pl.pallas_call(
        kernel,
        out_shape=(pltpu.VMEM(mixer_rows.shape, BF16), pltpu.VMEM(routed_rows.shape, BF16)),
        in_specs=[far] * 14,
        out_specs=(near, near),
        scratch_shapes=scratch,
        compiler_params=pltpu.CompilerParams(
            collective_id=0, has_side_effects=True, vmem_limit_bytes=60 * 1024 * 1024
        ),
        name="mixer_and_experts",
    )(
        mixer_rows, mixer_gain[None, :], inner_weight, gate_in_weight, gate_out_weight, conv_taps,
        mixer_out_weight, routed_rows, routed_gain[None, :], route_ids.T, route_weights.T,
        expert_gate[0], expert_up[0], expert_down[0],
    )
    return pl.pallas_call(
        store,
        out_shape=(
            jax.ShapeDtypeStruct(mixer_rows.shape, BF16),
            jax.ShapeDtypeStruct(routed_rows.shape, BF16),
        ),
        in_specs=[far, far],
        out_specs=(far, far),
        scratch_shapes=[pltpu.SemaphoreType.DMA((2,))],
        name="store",
    )(*(pltpu.with_memory_space_constraint(array, pltpu.VMEM) for array in done))


def solution(mesh):
    return jax.shard_map(
        on_device,
        mesh=mesh,
        in_specs=(
            P("ep", None), P(), P(None, "tp"), P(None, "tp"), P(None, "tp"), P(None, "tp"),
            P("tp", None), P("ep", None), P(), P("ep", None), P("ep", None),
            P("ep", None, "tp"), P("ep", None, "tp"), P("ep", "tp", None),
        ),
        out_specs=(P("ep", None), P("ep", None)),
        check_vma=False,
    )
```

```python
import jax
import jax.numpy as jnp
from jax import lax
from jax.experimental import pallas as pl
from jax.experimental.pallas import tpu as pltpu
from jax.sharding import PartitionSpec as P

F32, BF16, I32 = jnp.float32, jnp.bfloat16, jnp.int32
CORES = 2


def rms(values):
    return lax.rsqrt(jnp.mean(values * values, axis=-1, keepdims=True) + 1e-06)


def dot(a, b):
    return jnp.dot(a, b, preferred_element_type=F32)


ORDER = ("W", "C00", "E00", "M", "N", "A01", "Aa0", "O", "C01", "T", "Aa1", "Ba0", "Ca0", "Ea0", "A10", "Ab0", "P", "Ba1", "Ca1", "Ga0", "Ea1", "E01", "G00", "Ab1", "A11", "Bb0", "Cb0", "Eb0", "Ga1", "C10", "E10", "Bb1", "Cb1", "Gb00", "Eb1", "C11", "E11", "G01", "Gb10", "G100", "Gb01", "Gb11", "G110", "G101", "G111", "Gb02", "Gb12", "G102", "G112", "Gb03", "Gb13", "G103", "G113")
QUEUE = ("01", "20", "30", "21", "31", "10", "11")
KINDS = ("d1", "y", "b", "e", "g", "ret", "rim", "me", "mg", "ay", "ab")


def schedule(steps, per, whole):
    if steps == 4 and per == 2 and whole == 2:
        return 2, QUEUE, ORDER
    queue = [str(i) for i in range(steps)]
    order = ["M", "N", "T", "W", "A00", "C00", "O", "E00", "P"]
    for last, i in zip(queue, queue[1:]):
        order += [name + i + "0" for name in ("AC" if int(i) < whole else "ABC") + "E"]
        order.append("G" + last + "0")
    return 1, [i + "0" for i in queue], order + ["G" + queue[-1] + "0"]


def make_kernel(
    experts, groups, tok, picks, width, cap, steps, per, mrows, taps_n, chan, hid, whole, halves, queue, order, pieces
):
    high = groups // CORES
    slab = width // groups
    wide = slab // pieces
    size = per // halves
    rows = size * cap
    edge = 16 * -(-(taps_n - 1) // 16)

    def kernel(
        mixer_h, mixer_gain_h, inner_h, gate_in_h, gate_out_h, taps_h, mixer_out_h,
        routed_h, routed_gain_h, ids_h, weights_h, gate_h, up_h, down_h,
        out_m, out_r,
        mixer_rows, mixer_gain, taps, routed_rows, routed_gain, ids, weights,
        w_inner, w_gin, w_gout, w_mout, w_gate, w_up, w_down,
        disp, slots, part, r1, s2, r2, t3, ret,
        sums,
        rim, rim_in, m_part, m_r1, m_s2, m_r2,
        w_sem, own_sem, s_sem,
        d1_r, y_r, b_r, e_r, g_r, ret_r,
        rim_r, me_r, mg_r, ay_r, ab_r,
    ):
        me = lax.axis_index("ep")
        t = lax.axis_index("tp")
        yy, cc = t // CORES, t % CORES
        mate = yy * CORES + (1 - cc)
        my_chunk, my_j = me // per, me % per
        sent = {}

        def send(src, dst, kind, rsem, where):
            copy = pltpu.make_async_remote_copy(
                src_ref=src, dst_ref=dst, send_sem=s_sem.at[KINDS.index(kind)], recv_sem=rsem,
                device_id=where, device_id_type=pl.DeviceIdType.MESH,
            )
            copy.start()
            sent[kind] = sent.get(kind, 0) + volume(src.shape)

        def volume(shape):
            total = 1
            for n in shape:
                total *= n
            return total

        def carrier(count):
            for ref in (gate_h, disp, slots, part):
                line = volume(ref.shape[1:])
                if count % line == 0 and count // line <= ref.shape[0]:
                    return ref.at[0 : count // line]
            for ref in (disp, slots):
                for a in range(1, ref.shape[0] + 1):
                    line = a * volume(ref.shape[2:])
                    if count % line == 0 and count // line <= ref.shape[1]:
                        return ref.at[0:a, 0 : count // line]
            raise ValueError(count)

        def drain(*kinds):
            for kind in kinds:
                if kind in sent:
                    ref = carrier(sent.pop(kind))
                    pltpu.make_async_remote_copy(
                        src_ref=ref, dst_ref=ref, send_sem=s_sem.at[KINDS.index(kind)],
                        recv_sem=s_sem.at[KINDS.index(kind)],
                        device_id={"tp": mate}, device_id_type=pl.DeviceIdType.MESH,
                    ).wait_send()

        def arrive(dst, rsem):
            pltpu.make_async_remote_copy(
                src_ref=dst, dst_ref=dst, send_sem=s_sem.at[0], recv_sem=rsem,
                device_id={"tp": mate}, device_id_type=pl.DeviceIdType.MESH,
            ).wait_recv()

        def up_to(dy):
            return lax.rem(yy + dy, high)

        def down_to(dy):
            return lax.rem(yy + high - dy, high)

        barrier = pltpu.get_barrier_semaphore()
        for d in range(1, experts):
            pl.semaphore_signal(
                barrier, inc=1, device_id={"ep": lax.rem(me + d, experts)},
                device_id_type=pl.DeviceIdType.MESH,
            )
        for dy in range(1, high):
            pl.semaphore_signal(
                barrier, inc=1, device_id={"tp": up_to(dy) * CORES + cc},
                device_id_type=pl.DeviceIdType.MESH,
            )
        pl.semaphore_signal(
            barrier, inc=1, device_id={"tp": mate}, device_id_type=pl.DeviceIdType.MESH
        )

        loads = {}
        for place, (name, src, dst) in enumerate(
            (
                ("ids", ids_h, ids), ("weights", weights_h, weights),
                ("mixer", mixer_h, mixer_rows), ("mgain", mixer_gain_h, mixer_gain),
                ("gin", gate_in_h, w_gin), ("inner", inner_h, w_inner),
                ("routed", routed_h, routed_rows), ("rgain", routed_gain_h, routed_gain),
                ("taps", taps_h, taps), ("gout", gate_out_h, w_gout), ("mout", mixer_out_h, w_mout),
                ("gate", gate_h, w_gate), ("up", up_h, w_up), ("down", down_h, w_down),
            )
        ):
            loads[name] = pltpu.make_async_copy(src, dst, w_sem.at[place])
            loads[name].start()

        def loaded(*names):
            for name in names:
                loads[name].wait()

        with jax.named_scope("route"):
            loaded("ids", "weights")
            row = lax.broadcasted_iota(I32, (128, tok), 0)
            hits = [row == ids[k : k + 1, :] for k in range(picks)]
            named = sum(h.astype(F32) for h in hits)
            before = (
                lax.broadcasted_iota(I32, (tok, tok), 0) < lax.broadcasted_iota(I32, (tok, tok), 1)
            ).astype(F32).astype(BF16)
            earlier = dot(named.astype(BF16), before)
            slot_row = lax.broadcasted_iota(I32, (experts * cap, tok), 0)
            pick_map = jnp.zeros((experts * cap, tok), F32)
            placed = []
            for k in range(picks):
                rank = jnp.sum(jnp.where(hits[k], earlier, 0.0), axis=0, keepdims=True).astype(I32)
                placed.append(ids[k : k + 1, :] * cap + rank)
                pick_map = pick_map + jnp.where(slot_row == placed[k], 1.0, 0.0)
            pick_map = pick_map.astype(BF16)

        def weigh():
            slot_row = lax.broadcasted_iota(I32, (experts * cap, tok), 0)
            total = jnp.zeros((experts * cap, tok), F32)
            for k in range(picks):
                total = total + jnp.where(slot_row == placed[k], weights[k : k + 1, :], 0.0)
            sums[...] = total.T.astype(BF16)

        my_cols = pl.ds(pl.multiple_of(t * slab, slab), slab)

        with jax.named_scope("mix1"):
            loaded("mixer", "mgain", "gin", "inner")
            mixed = mixer_rows[...].astype(F32)
            mixed = ((mixed * rms(mixed)) * mixer_gain[...]).astype(BF16)
            conv_input = (dot(mixed, w_gin[...]) * dot(mixed, w_inner[...])).astype(BF16)
            rim[...] = conv_input[mrows - edge :]

        def normed(dy, scale):
            y = down_to(dy)
            cols = pl.ds(pl.multiple_of((y * CORES + cc) * slab, slab), slab)
            return ((routed_rows[:, cols].astype(F32) * scale) * routed_gain[:, cols]).astype(BF16)

        def pick(dy):
            disp[dy] = dot(pick_map, rows_of[dy]).astype(BF16).reshape(experts, cap, slab)

        with jax.named_scope("pick"):
            loaded("routed", "rgain")
            scale = rms(routed_rows[...].astype(F32))
            rows_of = [normed(dy, scale) for dy in range(high)]

        with jax.named_scope("barrier"):
            pl.semaphore_wait(barrier, experts - 1 + high - 1 + 1)
        send(rim, rim_in, "rim", rim_r.at[0], {"ep": lax.rem(me + 1, experts)})
        pick(0)

        def blocks(h):
            return [lax.rem(my_j + h * size + n, per) for n in range(size)]

        def is_own(i, h, n):
            return i == "0" and h == 0 and n == 0

        outer = 1 - (my_chunk + 1) // 2 % 2
        index = {"a": 2 + outer, "b": 3 - outer}

        def at(i):
            return index[i] if i in index else int(i)

        def far(i):
            return i in index or int(i) >= whole

        def partner(i):
            chunk, other = my_chunk, at(i)
            for bit in (1 << n for n in range((steps - 1).bit_length())):
                chunk = chunk + other // bit % 2 * (bit - 2 * bit * lax.rem(chunk // bit, 2))
            return chunk

        def slabs(i):
            return range(1 if far(i) else high)

        def dispatch(i, h):
            for n, jj in enumerate(blocks(h)):
                if not is_own(i, h, n):
                    dest = partner(i) * per + jj
                    for dy in slabs(i):
                        send(disp.at[dy, dest], slots.at[down_to(dy) * CORES + cc, at(i), my_j], "d1", d1_r.at[at(i), my_j], {"ep": dest})

        own = []

        def keep(dy):
            block = slots.at[down_to(dy) * CORES + cc, 0, my_j]
            send(disp.at[dy, me], block, "b", b_r.at[0, 0], {"tp": mate})
            copy = pltpu.make_async_copy(disp.at[dy, me], block, own_sem.at[dy])
            copy.start()
            own.append(copy)

        with jax.named_scope("dispatch"):
            keep(0)
            for dy in range(1, high):
                pick(dy)
                keep(dy)
            for word in queue:
                dispatch(word[0], int(word[1]))

        def stage_a(i, h):
            k = at(i)
            for n, jj in enumerate(blocks(h)):
                if is_own(i, h, n):
                    continue
                arrive(slots.at[0 : len(slabs(i)), k, jj], d1_r.at[k, jj])
                for dy in slabs(i):
                    block = slots.at[down_to(dy) * CORES + cc, k, jj]
                    if far(i):
                        for up in range(1, high):
                            send(
                                block, block, "y", y_r.at[k, up - 1, jj], {"tp": up_to(up) * CORES + cc}
                            )
                    send(block, block, "b", b_r.at[k, h], {"tp": mate})

        def stage_b(i, h):
            k = at(i)
            for dy in range(1, high):
                for jj in blocks(h):
                    block = slots.at[down_to(dy) * CORES + cc, k, jj]
                    arrive(block, y_r.at[k, dy - 1, jj])
                    send(block, block, "b", b_r.at[k, h], {"tp": mate})

        turns = list(range(1, high)) + [0]

        def columns(dy, core):
            return pl.ds(pl.multiple_of((up_to(dy) * CORES + core) * slab, slab), slab)

        def stage_c(i, h):
            k = at(i)
            arrive(slots.at[0:high, k, 0:size], b_r.at[k, h])
            if is_own(i, h, 0):
                for copy in own:
                    copy.wait()
            x = jnp.concatenate(
                [
                    jnp.concatenate([slots[q, k, jj] for q in range(groups)], axis=1)
                    for jj in blocks(h)
                ],
                axis=0,
            )
            gate, up = dot(x, w_gate[...]), dot(x, w_up[...])
            hidden = (gate / (1.0 + jnp.exp(-gate)) * up).astype(BF16)
            for side, core in ((0, 1 - cc), (1, cc)):
                for dy in turns:
                    value = dot(hidden, w_down[:, columns(dy, core)]).astype(BF16)
                    for p in range(pieces):
                        part[k, h, side, dy, p] = value[:, p * wide : (p + 1) * wide]
                    if side == 0:
                        send(part.at[k, h, 0, dy], r1.at[k, h, dy], "e", e_r.at[k, h, dy], {"tp": mate})

        def stage_e(i, h):
            k = at(i)
            for dy in range(1, high):
                arrive(r1.at[k, h, dy], e_r.at[k, h, dy])
                for p in range(pieces):
                    s2[k, h, dy - 1, p] = (
                        part[k, h, 1, dy, p].astype(F32) + r1[k, h, dy, p].astype(F32)
                    ).astype(BF16)
                    send(
                        s2.at[k, h, dy - 1, p], r2.at[k, h, dy - 1, p], "g", g_r.at[k, h, dy - 1, p],
                        {"tp": up_to(dy) * CORES + cc},
                    )

        def stage_g(i, h, *only):
            k = at(i)
            for p in only or range(pieces):
                if p == 0:
                    arrive(r1.at[k, h, 0], e_r.at[k, h, 0])
                total = part[k, h, 1, 0, p].astype(F32) + r1[k, h, 0, p].astype(F32)
                for dy in range(1, high):
                    arrive(r2.at[k, h, dy - 1, p], g_r.at[k, h, dy - 1, p])
                    total = total + r2[k, h, dy - 1, p].astype(F32)
                t3[k, h, p] = total.astype(BF16).reshape(size, cap, wide)
                for n, jj in enumerate(blocks(h)):
                    if is_own(i, h, n):
                        ret[p, me] = t3[k, h, p, n]
                        continue
                    dest = partner(i) * per + jj
                    send(t3.at[k, h, p, n], ret.at[p, me], "ret", ret_r.at[p], {"ep": dest})

        def window_of(out, group, p, count):
            span = slab // count
            return out.at[:, pl.ds(pl.multiple_of(group * slab + p * span, span), span)]

        def spread(which, out, p, count, value):
            span = slab // count
            out[:, pl.ds(pl.multiple_of(t * slab + p * span, span), span)] = value
            window = window_of(out, t, p, count)
            for dy in range(1, high):
                send(window, window, "ay", ay_r.at[which, dy - 1, p], {"tp": up_to(dy) * CORES + cc})
            send(window, window, "ab", ab_r.at[which], {"tp": mate})

        def spread_on(which, out, p, count):
            for dy in range(1, high):
                window = window_of(out, down_to(dy) * CORES + cc, p, count)
                arrive(window, ay_r.at[which, dy - 1, p])
                send(window, window, "ab", ab_r.at[which], {"tp": mate})

        def spread_end(which, out):
            arrive(out.at[:, pl.ds(0, high * slab)], ab_r.at[which])

        def mixer_out():
            loaded("gout", "taps")
            gate_out = dot(mixed, w_gout[...])
            arrive(rim_in, rim_r.at[0])
            first = jnp.where(me == 0, 0.0, rim_in[...].astype(F32))
            extended = jnp.concatenate([first, conv_input.astype(F32)], axis=0)
            conv = jnp.zeros((mrows, chan), F32)
            for k in range(taps_n):
                start = edge - (taps_n - 1) + k
                conv = conv + taps[k : k + 1, :] * extended[start : start + mrows]
            gated = (gate_out * conv).astype(BF16)
            loaded("mout")
            for side, core in ((0, 1 - cc), (1, cc)):
                for dy in turns:
                    m_part[side, dy] = dot(gated, w_mout[:, columns(dy, core)]).astype(BF16)
                    if side == 0:
                        send(m_part.at[0, dy], m_r1.at[dy], "me", me_r.at[dy], {"tp": mate})

        def mixer_pair():
            for dy in range(1, high):
                arrive(m_r1.at[dy], me_r.at[dy])
                m_s2[dy - 1] = (m_part[1, dy].astype(F32) + m_r1[dy].astype(F32)).astype(BF16)
                send(m_s2.at[dy - 1], m_r2.at[dy - 1], "mg", mg_r.at[dy - 1], {"tp": up_to(dy) * CORES + cc})

        def mixer_sum():
            arrive(m_r1.at[0], me_r.at[0])
            total = m_part[1, 0].astype(F32) + m_r1[0].astype(F32)
            for dy in range(1, high):
                arrive(m_r2.at[dy - 1], mg_r.at[dy - 1])
                total = total + m_r2[dy - 1].astype(F32)
            spread(0, out_m, 0, 1, total.astype(BF16))

        def finish(p):
            arrive(ret.at[p, 0 : experts - 1], ret_r.at[p])
            total = dot(sums[...], ret[p].reshape(experts * cap, wide))
            spread(1, out_r, p, pieces, total.astype(BF16))

        stages = dict(
            M=mixer_out, N=mixer_pair, O=mixer_sum, P=lambda: spread_on(0, out_m, 0, 1),
            W=lambda: loaded("gate", "up", "down"), T=weigh,
            A=stage_a, B=stage_b, C=stage_c, E=stage_e, G=stage_g,
        )
        for word in order:
            with jax.named_scope(word):
                stages[word[0]](*((word[1], *(int(c) for c in word[2:])) if word[1:] else ()))
        with jax.named_scope("early"):
            drain("d1", "y", "b", "e", "rim", "me", "mg")
        for p in range(pieces):
            with jax.named_scope("finish%d" % p):
                finish(p)
        with jax.named_scope("spreadon"):
            drain("g", "ret")
            for p in range(pieces):
                spread_on(1, out_r, p, pieces)
        with jax.named_scope("end"):
            spread_end(0, out_m)
            spread_end(1, out_r)
        with jax.named_scope("drain"):
            drain("ay", "ab")

    dma = pltpu.SemaphoreType.DMA
    far = max(1, high - 1)
    v = lambda *shape: pltpu.VMEM(shape, BF16)
    f = lambda *shape: pltpu.VMEM(shape, F32)
    scratch = [
        v(mrows, width), f(1, width), f(taps_n, chan), v(tok, width), f(1, width),
        pltpu.VMEM((picks, tok), I32), f(picks, tok),
        v(width, chan), v(width, chan), v(width, chan), v(chan, width),
        v(width, hid), v(width, hid), v(hid, width),
        v(high, experts, cap, slab), v(groups, steps, per, cap, slab),
        v(steps, halves, 2, high, pieces, rows, wide), v(steps, halves, high, pieces, rows, wide),
        v(steps, halves, far, pieces, rows, wide), v(steps, halves, far, pieces, rows, wide),
        v(steps, halves, pieces, size, cap, wide), v(pieces, experts, cap, wide),
        v(tok, experts * cap),
        v(edge, chan), v(edge, chan),
        v(2, high, mrows, slab), v(high, mrows, slab), v(far, mrows, slab), v(far, mrows, slab),
        dma((14,)), dma((high,)), dma((len(KINDS),)),
        dma((steps, per)), dma((steps, far, per)), dma((steps, halves)),
        dma((steps, halves, high)), dma((steps, halves, far, pieces)), dma((pieces,)),
        dma((1,)), dma((high,)), dma((far,)), dma((2, far, pieces)), dma((2,)),
    ]
    return kernel, scratch


def store(a, b, out_a, out_b, sem):
    copies = [
        pltpu.make_async_copy(a, out_a, sem.at[0]), pltpu.make_async_copy(b, out_b, sem.at[1])
    ]
    for copy in copies:
        copy.start()
    for copy in copies:
        copy.wait()


def on_device(
    mixer_rows, mixer_gain, inner_weight, gate_in_weight, gate_out_weight, conv_taps,
    mixer_out_weight, routed_rows, routed_gain, route_ids, route_weights,
    expert_gate, expert_up, expert_down,
):
    experts, groups = lax.axis_size("ep"), lax.axis_size("tp")
    tok, picks = route_ids.shape
    width = routed_rows.shape[1]
    cap = 2 * tok * picks // experts
    per = max(1, min(experts, tok // cap))
    steps = experts // per
    mrows = mixer_rows.shape[0]
    taps_n, chan = conv_taps.shape
    whole = 2 if groups // CORES == 2 else 1
    pieces = max(1, min(4, width // groups // 128))
    kernel, scratch = make_kernel(
        experts, groups, tok, picks, width, cap, steps, per, mrows, taps_n, chan,
        expert_gate.shape[2], whole, *schedule(steps, per, whole), pieces,
    )
    near, far = pl.BlockSpec(memory_space=pltpu.VMEM), pl.BlockSpec(memory_space=pl.ANY)
    done = pl.pallas_call(
        kernel,
        out_shape=(pltpu.VMEM(mixer_rows.shape, BF16), pltpu.VMEM(routed_rows.shape, BF16)),
        in_specs=[far] * 14,
        out_specs=(near, near),
        scratch_shapes=scratch,
        compiler_params=pltpu.CompilerParams(
            collective_id=0, has_side_effects=True, vmem_limit_bytes=60 * 1024 * 1024
        ),
        name="mixer_and_experts",
    )(
        mixer_rows, mixer_gain[None, :], inner_weight, gate_in_weight, gate_out_weight, conv_taps,
        mixer_out_weight, routed_rows, routed_gain[None, :], route_ids.T, route_weights.T,
        expert_gate[0], expert_up[0], expert_down[0],
    )
    return pl.pallas_call(
        store,
        out_shape=(
            jax.ShapeDtypeStruct(mixer_rows.shape, BF16),
            jax.ShapeDtypeStruct(routed_rows.shape, BF16),
        ),
        in_specs=[far, far],
        out_specs=(far, far),
        scratch_shapes=[pltpu.SemaphoreType.DMA((2,))],
        name="store",
    )(*(pltpu.with_memory_space_constraint(array, pltpu.VMEM) for array in done))


def solution(mesh):
    return jax.shard_map(
        on_device,
        mesh=mesh,
        in_specs=(
            P("ep", None), P(), P(None, "tp"), P(None, "tp"), P(None, "tp"), P(None, "tp"),
            P("tp", None), P("ep", None), P(), P("ep", None), P("ep", None),
            P("ep", None, "tp"), P("ep", None, "tp"), P("ep", "tp", None),
        ),
        out_specs=(P("ep", None), P("ep", None)),
        check_vma=False,
    )
```

```python
import jax
import jax.numpy as jnp
from jax import lax
from jax.experimental import pallas as pl
from jax.experimental.pallas import tpu as pltpu
from jax.sharding import PartitionSpec as P

F32, BF16, I32 = jnp.float32, jnp.bfloat16, jnp.int32
CORES = 2


def rms(values):
    return lax.rsqrt(jnp.mean(values * values, axis=-1, keepdims=True) + 1e-06)


def dot(a, b):
    return jnp.dot(a, b, preferred_element_type=F32)


ORDER = (
    "W", "C00", "E00", "M", "N", "A01", "Aa0", "C01", "O", "T",
    "Ba0", "Aa1", "Ca0", "Ea0", "A10", "Ba1", "Ab0", "P", "Ca1", "Ga0",
    "Ea1", "E01", "G00", "Bb0", "Ab1", "A11", "Cb0", "Ga1", "Eb0", "C10",
    "Bb1", "E10", "Cb1", "Gb00", "Gb01", "Eb1", "C11", "E11", "G01", "Gb10",
    "G100", "Gb11", "G110", "Gb02", "G101", "G111", "Gb12", "G102", "G112", "Gb03",
    "Gb13", "G103", "G113",
)
QUEUE = ("01", "20", "30", "21", "31", "10", "11")
KINDS = ("d1", "y", "b", "e", "g", "ret", "rim", "me", "mg", "ay", "ab")


def schedule(steps, per, whole):
    if steps == 4 and per == 2 and whole == 2:
        return 2, QUEUE, ORDER
    queue = [str(i) for i in range(steps)]
    order = ["M", "N", "T", "W", "A00", "C00", "O", "E00", "P"]
    for last, i in zip(queue, queue[1:]):
        order += [name + i + "0" for name in ("AC" if int(i) < whole else "ABC") + "E"]
        order.append("G" + last + "0")
    return 1, [i + "0" for i in queue], order + ["G" + queue[-1] + "0"]


def make_kernel(
    experts, groups, tok, picks, width, cap, steps, per, mrows, taps_n, chan, hid, whole, halves, queue, order, pieces
):
    high = groups // CORES
    slab = width // groups
    wide = slab // pieces
    size = per // halves
    rows = size * cap
    edge = 16 * -(-(taps_n - 1) // 16)

    def kernel(
        mixer_h, mixer_gain_h, inner_h, gate_in_h, gate_out_h, taps_h, mixer_out_h,
        routed_h, routed_gain_h, ids_h, weights_h, gate_h, up_h, down_h,
        out_m, out_r,
        mixer_rows, mixer_gain, taps, routed_rows, routed_gain, ids, weights,
        w_inner, w_gin, w_gout, w_mout, w_gate, w_up, w_down,
        disp, slots, part, r1, s2, r2, t3, ret,
        sums,
        rim, rim_in, m_part, m_r1, m_s2, m_r2,
        w_sem, own_sem, s_sem,
        d1_r, y_r, b_r, e_r, g_r, ret_r,
        rim_r, me_r, mg_r, ay_r, ab_r,
    ):
        me = lax.axis_index("ep")
        t = lax.axis_index("tp")
        yy, cc = t // CORES, t % CORES
        mate = yy * CORES + (1 - cc)
        my_chunk, my_j = me // per, me % per
        sent = {}

        def send(src, dst, kind, rsem, where):
            copy = pltpu.make_async_remote_copy(
                src_ref=src, dst_ref=dst, send_sem=s_sem.at[KINDS.index(kind)], recv_sem=rsem,
                device_id=where, device_id_type=pl.DeviceIdType.MESH,
            )
            copy.start()
            sent[kind] = sent.get(kind, 0) + volume(src.shape)

        def volume(shape):
            total = 1
            for n in shape:
                total *= n
            return total

        def carrier(count):
            for ref in (gate_h, disp, slots, part):
                line = volume(ref.shape[1:])
                if count % line == 0 and count // line <= ref.shape[0]:
                    return ref.at[0 : count // line]
            for ref in (disp, slots):
                for a in range(1, ref.shape[0] + 1):
                    line = a * volume(ref.shape[2:])
                    if count % line == 0 and count // line <= ref.shape[1]:
                        return ref.at[0:a, 0 : count // line]
            raise ValueError(count)

        def drain(*kinds):
            for kind in kinds:
                if kind in sent:
                    ref = carrier(sent.pop(kind))
                    pltpu.make_async_remote_copy(
                        src_ref=ref, dst_ref=ref, send_sem=s_sem.at[KINDS.index(kind)],
                        recv_sem=s_sem.at[KINDS.index(kind)],
                        device_id={"tp": mate}, device_id_type=pl.DeviceIdType.MESH,
                    ).wait_send()

        def arrive(dst, rsem):
            pltpu.make_async_remote_copy(
                src_ref=dst, dst_ref=dst, send_sem=s_sem.at[0], recv_sem=rsem,
                device_id={"tp": mate}, device_id_type=pl.DeviceIdType.MESH,
            ).wait_recv()

        def up_to(dy):
            return lax.rem(yy + dy, high)

        def down_to(dy):
            return lax.rem(yy + high - dy, high)

        barrier = pltpu.get_barrier_semaphore()
        for d in range(1, experts):
            pl.semaphore_signal(
                barrier, inc=1, device_id={"ep": lax.rem(me + d, experts)},
                device_id_type=pl.DeviceIdType.MESH,
            )
        for dy in range(1, high):
            pl.semaphore_signal(
                barrier, inc=1, device_id={"tp": up_to(dy) * CORES + cc},
                device_id_type=pl.DeviceIdType.MESH,
            )
        pl.semaphore_signal(
            barrier, inc=1, device_id={"tp": mate}, device_id_type=pl.DeviceIdType.MESH
        )

        loads = {}
        for place, (name, src, dst) in enumerate(
            (
                ("ids", ids_h, ids), ("weights", weights_h, weights),
                ("mixer", mixer_h, mixer_rows), ("mgain", mixer_gain_h, mixer_gain),
                ("gin", gate_in_h, w_gin), ("inner", inner_h, w_inner),
                ("routed", routed_h, routed_rows), ("rgain", routed_gain_h, routed_gain),
                ("taps", taps_h, taps), ("gout", gate_out_h, w_gout), ("mout", mixer_out_h, w_mout),
                ("gate", gate_h, w_gate), ("up", up_h, w_up), ("down", down_h, w_down),
            )
        ):
            loads[name] = pltpu.make_async_copy(src, dst, w_sem.at[place])
            loads[name].start()

        def loaded(*names):
            for name in names:
                loads[name].wait()

        with jax.named_scope("route"):
            loaded("ids", "weights")
            row = lax.broadcasted_iota(I32, (128, tok), 0)
            hits = [row == ids[k : k + 1, :] for k in range(picks)]
            named = sum(h.astype(F32) for h in hits)
            before = (
                lax.broadcasted_iota(I32, (tok, tok), 0) < lax.broadcasted_iota(I32, (tok, tok), 1)
            ).astype(F32).astype(BF16)
            earlier = dot(named.astype(BF16), before)
            slot_row = lax.broadcasted_iota(I32, (experts * cap, tok), 0)
            pick_map = jnp.zeros((experts * cap, tok), F32)
            placed = []
            for k in range(picks):
                rank = jnp.sum(jnp.where(hits[k], earlier, 0.0), axis=0, keepdims=True).astype(I32)
                placed.append(ids[k : k + 1, :] * cap + rank)
                pick_map = pick_map + jnp.where(slot_row == placed[k], 1.0, 0.0)
            pick_map = pick_map.astype(BF16)

        def weigh():
            slot_row = lax.broadcasted_iota(I32, (experts * cap, tok), 0)
            total = jnp.zeros((experts * cap, tok), F32)
            for k in range(picks):
                total = total + jnp.where(slot_row == placed[k], weights[k : k + 1, :], 0.0)
            sums[...] = total.T.astype(BF16)

        my_cols = pl.ds(pl.multiple_of(t * slab, slab), slab)

        with jax.named_scope("mix1"):
            loaded("mixer", "mgain", "gin", "inner")
            mixed = mixer_rows[...].astype(F32)
            mixed = ((mixed * rms(mixed)) * mixer_gain[...]).astype(BF16)
            conv_input = (dot(mixed, w_gin[...]) * dot(mixed, w_inner[...])).astype(BF16)
            rim[...] = conv_input[mrows - edge :]

        def normed(dy, scale):
            y = down_to(dy)
            cols = pl.ds(pl.multiple_of((y * CORES + cc) * slab, slab), slab)
            return ((routed_rows[:, cols].astype(F32) * scale) * routed_gain[:, cols]).astype(BF16)

        def pick(dy):
            disp[dy] = dot(pick_map, rows_of[dy]).astype(BF16).reshape(experts, cap, slab)

        with jax.named_scope("pick"):
            loaded("routed", "rgain")
            scale = rms(routed_rows[...].astype(F32))
            rows_of = [normed(dy, scale) for dy in range(high)]

        with jax.named_scope("barrier"):
            pl.semaphore_wait(barrier, experts - 1 + high - 1 + 1)
        send(rim, rim_in, "rim", rim_r.at[0], {"ep": lax.rem(me + 1, experts)})
        pick(0)

        def blocks(h):
            return [lax.rem(my_j + h * size + n, per) for n in range(size)]

        def is_own(i, h, n):
            return i == "0" and h == 0 and n == 0

        outer = 1 - (my_chunk + 1) // 2 % 2
        index = {"a": 2 + outer, "b": 3 - outer}

        def at(i):
            return index[i] if i in index else int(i)

        def far(i):
            return i in index or int(i) >= whole

        def partner(i):
            chunk, other = my_chunk, at(i)
            for bit in (1 << n for n in range((steps - 1).bit_length())):
                chunk = chunk + other // bit % 2 * (bit - 2 * bit * lax.rem(chunk // bit, 2))
            return chunk

        def slabs(i):
            return range(1 if far(i) else high)

        def dispatch(i, h):
            for n, jj in enumerate(blocks(h)):
                if not is_own(i, h, n):
                    dest = partner(i) * per + jj
                    for dy in slabs(i):
                        send(disp.at[dy, dest], slots.at[down_to(dy) * CORES + cc, at(i), my_j], "d1", d1_r.at[at(i), my_j], {"ep": dest})

        own = []

        def keep(dy):
            block = slots.at[down_to(dy) * CORES + cc, 0, my_j]
            send(disp.at[dy, me], block, "b", b_r.at[0, 0], {"tp": mate})
            copy = pltpu.make_async_copy(disp.at[dy, me], block, own_sem.at[dy])
            copy.start()
            own.append(copy)

        with jax.named_scope("dispatch"):
            keep(0)
            for dy in range(1, high):
                pick(dy)
                keep(dy)
            for word in queue:
                dispatch(word[0], int(word[1]))

        def stage_a(i, h):
            k = at(i)
            for n, jj in enumerate(blocks(h)):
                if is_own(i, h, n):
                    continue
                arrive(slots.at[0 : len(slabs(i)), k, jj], d1_r.at[k, jj])
                for dy in slabs(i):
                    block = slots.at[down_to(dy) * CORES + cc, k, jj]
                    if far(i):
                        for up in range(1, high):
                            send(
                                block, block, "y", y_r.at[k, up - 1, jj], {"tp": up_to(up) * CORES + cc}
                            )
                    send(block, block, "b", b_r.at[k, h], {"tp": mate})

        def stage_b(i, h):
            k = at(i)
            for dy in range(1, high):
                for jj in blocks(h):
                    block = slots.at[down_to(dy) * CORES + cc, k, jj]
                    arrive(block, y_r.at[k, dy - 1, jj])
                    send(block, block, "b", b_r.at[k, h], {"tp": mate})

        turns = list(range(1, high)) + [0]

        def columns(dy, core):
            return pl.ds(pl.multiple_of((up_to(dy) * CORES + core) * slab, slab), slab)

        def stage_c(i, h):
            k = at(i)
            arrive(slots.at[0:high, k, 0:size], b_r.at[k, h])
            if is_own(i, h, 0):
                for copy in own:
                    copy.wait()
            x = jnp.concatenate(
                [
                    jnp.concatenate([slots[q, k, jj] for q in range(groups)], axis=1)
                    for jj in blocks(h)
                ],
                axis=0,
            )
            gate, up = dot(x, w_gate[...]), dot(x, w_up[...])
            hidden = (gate / (1.0 + jnp.exp(-gate)) * up).astype(BF16)
            for side, core in ((0, 1 - cc), (1, cc)):
                for dy in turns:
                    value = dot(hidden, w_down[:, columns(dy, core)]).astype(BF16)
                    for p in range(pieces):
                        part[k, h, side, dy, p] = value[:, p * wide : (p + 1) * wide]
                    if side == 0:
                        send(part.at[k, h, 0, dy], r1.at[k, h, dy], "e", e_r.at[k, h, dy], {"tp": mate})

        def stage_e(i, h):
            k = at(i)
            for dy in range(1, high):
                arrive(r1.at[k, h, dy], e_r.at[k, h, dy])
                for p in range(pieces):
                    s2[k, h, dy - 1, p] = (
                        part[k, h, 1, dy, p].astype(F32) + r1[k, h, dy, p].astype(F32)
                    ).astype(BF16)
                    send(
                        s2.at[k, h, dy - 1, p], r2.at[k, h, dy - 1, p], "g", g_r.at[k, h, dy - 1, p],
                        {"tp": up_to(dy) * CORES + cc},
                    )

        def stage_g(i, h, *only):
            k = at(i)
            for p in only or range(pieces):
                if p == 0:
                    arrive(r1.at[k, h, 0], e_r.at[k, h, 0])
                total = part[k, h, 1, 0, p].astype(F32) + r1[k, h, 0, p].astype(F32)
                for dy in range(1, high):
                    arrive(r2.at[k, h, dy - 1, p], g_r.at[k, h, dy - 1, p])
                    total = total + r2[k, h, dy - 1, p].astype(F32)
                t3[k, h, p] = total.astype(BF16).reshape(size, cap, wide)
                for n, jj in enumerate(blocks(h)):
                    if is_own(i, h, n):
                        ret[p, me] = t3[k, h, p, n]
                        continue
                    dest = partner(i) * per + jj
                    send(t3.at[k, h, p, n], ret.at[p, me], "ret", ret_r.at[p], {"ep": dest})

        def window_of(out, group, p, count):
            span = slab // count
            return out.at[:, pl.ds(pl.multiple_of(group * slab + p * span, span), span)]

        def spread(which, out, p, count, value):
            span = slab // count
            out[:, pl.ds(pl.multiple_of(t * slab + p * span, span), span)] = value
            window = window_of(out, t, p, count)
            for dy in range(1, high):
                send(window, window, "ay", ay_r.at[which, dy - 1, p], {"tp": up_to(dy) * CORES + cc})
            send(window, window, "ab", ab_r.at[which], {"tp": mate})

        def spread_on(which, out, p, count):
            for dy in range(1, high):
                window = window_of(out, down_to(dy) * CORES + cc, p, count)
                arrive(window, ay_r.at[which, dy - 1, p])
                send(window, window, "ab", ab_r.at[which], {"tp": mate})

        def spread_end(which, out):
            arrive(out.at[:, pl.ds(0, high * slab)], ab_r.at[which])

        def mixer_out():
            loaded("gout", "taps")
            gate_out = dot(mixed, w_gout[...])
            arrive(rim_in, rim_r.at[0])
            first = jnp.where(me == 0, 0.0, rim_in[...].astype(F32))
            extended = jnp.concatenate([first, conv_input.astype(F32)], axis=0)
            conv = jnp.zeros((mrows, chan), F32)
            for k in range(taps_n):
                start = edge - (taps_n - 1) + k
                conv = conv + taps[k : k + 1, :] * extended[start : start + mrows]
            gated = (gate_out * conv).astype(BF16)
            loaded("mout")
            for side, core in ((0, 1 - cc), (1, cc)):
                for dy in turns:
                    m_part[side, dy] = dot(gated, w_mout[:, columns(dy, core)]).astype(BF16)
                    if side == 0:
                        send(m_part.at[0, dy], m_r1.at[dy], "me", me_r.at[dy], {"tp": mate})

        def mixer_pair():
            for dy in range(1, high):
                arrive(m_r1.at[dy], me_r.at[dy])
                m_s2[dy - 1] = (m_part[1, dy].astype(F32) + m_r1[dy].astype(F32)).astype(BF16)
                send(m_s2.at[dy - 1], m_r2.at[dy - 1], "mg", mg_r.at[dy - 1], {"tp": up_to(dy) * CORES + cc})

        def mixer_sum():
            arrive(m_r1.at[0], me_r.at[0])
            total = m_part[1, 0].astype(F32) + m_r1[0].astype(F32)
            for dy in range(1, high):
                arrive(m_r2.at[dy - 1], mg_r.at[dy - 1])
                total = total + m_r2[dy - 1].astype(F32)
            spread(0, out_m, 0, 1, total.astype(BF16))

        def finish(p):
            arrive(ret.at[p, 0 : experts - 1], ret_r.at[p])
            total = dot(sums[...], ret[p].reshape(experts * cap, wide))
            spread(1, out_r, p, pieces, total.astype(BF16))

        stages = dict(
            M=mixer_out, N=mixer_pair, O=mixer_sum, P=lambda: spread_on(0, out_m, 0, 1),
            W=lambda: loaded("gate", "up", "down"), T=weigh,
            A=stage_a, B=stage_b, C=stage_c, E=stage_e, G=stage_g,
        )
        for word in order:
            with jax.named_scope(word):
                stages[word[0]](*((word[1], *(int(c) for c in word[2:])) if word[1:] else ()))
        with jax.named_scope("early"):
            drain("d1", "y", "b", "e", "rim", "me", "mg")
        for p in range(pieces):
            with jax.named_scope("finish%d" % p):
                finish(p)
        with jax.named_scope("spreadon"):
            drain("g", "ret")
            for p in range(pieces):
                spread_on(1, out_r, p, pieces)
        with jax.named_scope("end"):
            spread_end(0, out_m)
            spread_end(1, out_r)
        with jax.named_scope("drain"):
            drain("ay", "ab")

    dma = pltpu.SemaphoreType.DMA
    far = max(1, high - 1)
    v = lambda *shape: pltpu.VMEM(shape, BF16)
    f = lambda *shape: pltpu.VMEM(shape, F32)
    scratch = [
        v(mrows, width), f(1, width), f(taps_n, chan), v(tok, width), f(1, width),
        pltpu.VMEM((picks, tok), I32), f(picks, tok),
        v(width, chan), v(width, chan), v(width, chan), v(chan, width),
        v(width, hid), v(width, hid), v(hid, width),
        v(high, experts, cap, slab), v(groups, steps, per, cap, slab),
        v(steps, halves, 2, high, pieces, rows, wide), v(steps, halves, high, pieces, rows, wide),
        v(steps, halves, far, pieces, rows, wide), v(steps, halves, far, pieces, rows, wide),
        v(steps, halves, pieces, size, cap, wide), v(pieces, experts, cap, wide),
        v(tok, experts * cap),
        v(edge, chan), v(edge, chan),
        v(2, high, mrows, slab), v(high, mrows, slab), v(far, mrows, slab), v(far, mrows, slab),
        dma((14,)), dma((high,)), dma((len(KINDS),)),
        dma((steps, per)), dma((steps, far, per)), dma((steps, halves)),
        dma((steps, halves, high)), dma((steps, halves, far, pieces)), dma((pieces,)),
        dma((1,)), dma((high,)), dma((far,)), dma((2, far, pieces)), dma((2,)),
    ]
    return kernel, scratch


def store(a, b, out_a, out_b, sem):
    copies = [
        pltpu.make_async_copy(a, out_a, sem.at[0]), pltpu.make_async_copy(b, out_b, sem.at[1])
    ]
    for copy in copies:
        copy.start()
    for copy in copies:
        copy.wait()


def on_device(
    mixer_rows, mixer_gain, inner_weight, gate_in_weight, gate_out_weight, conv_taps,
    mixer_out_weight, routed_rows, routed_gain, route_ids, route_weights,
    expert_gate, expert_up, expert_down,
):
    experts, groups = lax.axis_size("ep"), lax.axis_size("tp")
    tok, picks = route_ids.shape
    width = routed_rows.shape[1]
    cap = 2 * tok * picks // experts
    per = max(1, min(experts, tok // cap))
    steps = experts // per
    mrows = mixer_rows.shape[0]
    taps_n, chan = conv_taps.shape
    whole = 2 if groups // CORES == 2 else 1
    pieces = max(1, min(4, width // groups // 128))
    kernel, scratch = make_kernel(
        experts, groups, tok, picks, width, cap, steps, per, mrows, taps_n, chan,
        expert_gate.shape[2], whole, *schedule(steps, per, whole), pieces,
    )
    near, far = pl.BlockSpec(memory_space=pltpu.VMEM), pl.BlockSpec(memory_space=pl.ANY)
    done = pl.pallas_call(
        kernel,
        out_shape=(pltpu.VMEM(mixer_rows.shape, BF16), pltpu.VMEM(routed_rows.shape, BF16)),
        in_specs=[far] * 14,
        out_specs=(near, near),
        scratch_shapes=scratch,
        compiler_params=pltpu.CompilerParams(
            collective_id=0, has_side_effects=True, vmem_limit_bytes=60 * 1024 * 1024
        ),
        name="mixer_and_experts",
    )(
        mixer_rows, mixer_gain[None, :], inner_weight, gate_in_weight, gate_out_weight, conv_taps,
        mixer_out_weight, routed_rows, routed_gain[None, :], route_ids.T, route_weights.T,
        expert_gate[0], expert_up[0], expert_down[0],
    )
    return pl.pallas_call(
        store,
        out_shape=(
            jax.ShapeDtypeStruct(mixer_rows.shape, BF16),
            jax.ShapeDtypeStruct(routed_rows.shape, BF16),
        ),
        in_specs=[far, far],
        out_specs=(far, far),
        scratch_shapes=[pltpu.SemaphoreType.DMA((2,))],
        name="store",
    )(*(pltpu.with_memory_space_constraint(array, pltpu.VMEM) for array in done))


def solution(mesh):
    return jax.shard_map(
        on_device,
        mesh=mesh,
        in_specs=(
            P("ep", None), P(), P(None, "tp"), P(None, "tp"), P(None, "tp"), P(None, "tp"),
            P("tp", None), P("ep", None), P(), P("ep", None), P("ep", None),
            P("ep", None, "tp"), P("ep", None, "tp"), P("ep", "tp", None),
        ),
        out_specs=(P("ep", None), P("ep", None)),
        check_vma=False,
    )
```
